256 devices in a mesh: ep: 64 (over z, y, core), tp: 4 (over x).
Axes of the slice: x: 4, y: 4, z: 8, core: 2. Of those that a mesh axis runs over, the one named last changes fastest.
Arguments:
- tokens: bfloat16 [1024, 2048], P('ep'), may hold values from -6 to 6
- lengths: int32 [1024], P('ep'), may hold values from 256 to 1023
- cache: bfloat16 [1024, 1024, 512], P('ep', None, 'tp'), may hold values from -6 to 6
- attn_gain: float32 [2048], replicated, may hold values from 0.1 to 1.9
- query_weight: bfloat16 [2048, 1024], P(None, 'tp'), may hold values from -0.125 to 0.125
- key_weight: bfloat16 [2048, 256], P(None, 'tp'), may hold values from -0.125 to 0.125
- value_weight: bfloat16 [2048, 256], P(None, 'tp'), may hold values from -0.125 to 0.125
- stick_bias: float32 [16], P('tp'), may hold values from -7 to -1
- out_weight: bfloat16 [1024, 2048], P('tp'), may hold values from -0.1875 to 0.1875
- ffn_gain: float32 [2048], replicated, may hold values from 0.1 to 1.9
- routes: int32 [1024, 6], P('ep'), may hold values from 0 to 63, all different within a row; in each aligned block of 16 rows (0 to 15, 16 to 31, ...) at most 3 rows name the same one
- route_weights: float32 [1024, 6], P('ep'), may hold values from 0.1 to 0.6
- expert_gate: bfloat16 [64, 2048, 1024], P('ep', None, 'tp'), may hold values from -0.125 to 0.125
- expert_up: bfloat16 [64, 2048, 1024], P('ep', None, 'tp'), may hold values from -0.125 to 0.125
- expert_down: bfloat16 [64, 1024, 2048], P('ep', 'tp'), may hold values from -0.1875 to 0.1875
- shared_gate: bfloat16 [2048, 512], P('ep', 'tp'), may hold values from -0.125 to 0.125
- shared_up: bfloat16 [2048, 512], P('ep', 'tp'), may hold values from -0.125 to 0.125
- shared_down: bfloat16 [512, 2048], P('tp'), may hold values from -0.25 to 0.25
- gate_vector: bfloat16 [2048], replicated, may hold values from -0.125 to 0.125
Outputs:
- layer_out: bfloat16 [1024, 2048], P('ep', 'tp')
- new_kv: bfloat16 [1024, 512], P('ep', 'tp')
The draws below stay inside these ranges and needn't reach their ends.
Inputs may be any that keep to these rules, and one draw needn't show every extreme that they name: Each sequence's new token comes after its lengths cached positions. `routes`: each row names 6 different experts; among the 16 rows of one index of ep no expert is named by more than 3 rows.
All inputs are finite; a program needn't handle non-finite values.
Results may differ from the reference program's by a relative error of at most 0.012.
Values may be sent and summed in bfloat16 or wider, within the bound.
No kernel may reach another device: no remote copies, remote signals or barrier semaphores. Data moves between devices by JAX's collectives and lax.ppermute only.
A program may use at most 64 MiB of HBM per device.

```python
import math
import jax
import jax.numpy as jnp
import numpy as np
from jax import lax

D = 2048
HEAD_DIM = 64
Q_HEADS = 16
KV_HEADS = 4
EXPERT_FF = 1024
SHARED_FF = 512
TOP_K = 6
SEQ_DEV = 16
CACHE = 1024
SEQS = 1024
EXPERTS = 64
CAP = 3
N_EP = 64
N_TP = 4


def touch_ends(entries, own_key, low, largest):
    shape = entries.shape
    index_at = [jax.random.randint(jax.random.fold_in(own_key, axis), (), 0, shape[axis]) for axis in range(len(shape))]
    entries = entries.at[tuple(index_at)].set(low)
    longest = shape.index(max(shape))
    index_at[longest] = (index_at[longest] + 1) % shape[longest]
    return entries.at[tuple(index_at)].set(largest)


def steps_of(stream_key, dims, cuts, low, largest):
    def one(axis_at, parts):
        steps = jax.random.uniform(jax.random.fold_in(jax.random.fold_in(stream_key, 6), axis_at), (parts,), jnp.float32, low / len(cuts), largest / len(cuts))
        return jnp.repeat(jnp.exp(steps), dims[axis_at] // parts).reshape((-1,) + (1,) * (len(dims) - axis_at - 1))

    factor_of = one(*cuts[0])
    for cut in cuts[1:]:
        factor_of = factor_of * one(*cut)
    return factor_of


def routed_block(rng, own, number, rows, count, top, bound, lean):
    sequence = jax.random.permutation(rng, count)
    heavy_load, usual = shares(count, rows * top, bound, lean, True), shares(count, rows * top, bound, lean, False)
    places = jnp.arange(count)

    def named(tallies, turn):
        used = int((tallies > 0).sum())
        fixed = max(1, used // 4)
        passed = fixed + (places - fixed + turn * (used - fixed)) % max(1, count - fixed)
        return jnp.zeros((count,), jnp.int32).at[sequence[jnp.where(places < fixed, places, passed)]].set(jnp.asarray(tallies, jnp.int32))

    tallies = jnp.where(number % 4 == 0, named(heavy_load, number // 4), named(usual, number - number // 4 - 1))
    mixed = jax.random.permutation(jax.random.fold_in(own, 3), count)
    source_of, sink = mixed[0:count // 2 * 2:2], mixed[1:count // 2 * 2:2]
    slack = jnp.minimum(tallies[source_of] - 1, bound - tallies[sink]) // 2
    slack = jnp.where((source_of == sequence[0]) | (sink == sequence[0]) | (tallies[sink] == 0), 0, jnp.maximum(slack, 0))
    passed = jax.random.randint(jax.random.fold_in(own, 4), (count // 2,), 0, 1 << 20) % (slack + 1)
    tallies = tallies.at[source_of].add(-passed).at[sink].add(passed)
    items = jnp.searchsorted(jnp.cumsum(tallies), jnp.arange(rows * top), side="right").astype(jnp.int32)
    table = items.reshape(top, rows).T
    table = table[jax.random.permutation(jax.random.fold_in(own, 1), rows)]
    turn = jax.random.randint(jax.random.fold_in(own, 2), (rows, 1), 0, top)
    return jnp.take_along_axis(table, (jnp.arange(top)[None, :] + turn) % top, axis=1)


def shares(count, total, most, skew, full):
    loads = [(1 << 20) // math.isqrt(standing ** skew) + 1 for standing in range(1, count + 1)]
    largest = most if full else min(most, max(-(-total // count), total * loads[0] // sum(loads)))
    least = 1 if total - largest >= count - 1 else 0
    given, surplus = [largest] + [least] * (count - 1), total - largest - least * (count - 1)
    while surplus > 0:
        free = [i for i in range(1, count) if given[i] < largest] or [i for i in range(1, count) if given[i] < most]
        pool, remaining = sum([loads[i] for i in free]), surplus
        for i in free:
            addition = min(most - given[i], max(1, remaining * loads[i] // pool), surplus)
            given[i] = given[i] + addition
            surplus = surplus - addition
    return np.array(given)


def noise(rng, shape, spread, most, shards=(), kind=jnp.bfloat16):
    values = jax.random.normal(rng, shape, jnp.float32) * spread
    if len(shards) > 0:
        values = steps_of(rng, shape, shards, -0.22, 0.18) * values
    return jnp.clip(values, min=-most, max=most).astype(kind)


def setup_inputs(seed: int = 0) -> dict:
    splits = jax.random.split(jax.random.key(seed), 20)
    tokens = noise(splits[0], (SEQS, D), 1.0, 6.0, ((0, 64),))
    lengths = touch_ends(jax.random.randint(splits[1], (SEQS,), CACHE // 4, CACHE), jax.random.fold_in(splits[1], 1), CACHE // 4, CACHE - 1).astype(jnp.int32)
    cache = noise(splits[2], (SEQS, CACHE, 2 * KV_HEADS * HEAD_DIM), 1.0, 6.0, ((0, 64), (2, 4)))
    attn_gain = jnp.clip(1.0 + 0.18 * jax.random.normal(splits[3], (D,), jnp.float32), 0.1, 1.9)
    query_weight = noise(splits[4], (D, Q_HEADS * HEAD_DIM), D ** -0.5, 0.125, ((1, 4),))
    key_weight = noise(splits[5], (D, KV_HEADS * HEAD_DIM), D ** -0.5, 0.125, ((1, 4),))
    value_weight = noise(splits[6], (D, KV_HEADS * HEAD_DIM), D ** -0.5, 0.125, ((1, 4),))
    stick_bias = jnp.clip(-7.0 + 6.0 * jax.random.uniform(splits[7], (Q_HEADS,), jnp.float32) ** steps_of(splits[7], (Q_HEADS,), ((0, 4),), -0.2, 0.2), -7.0, -1.0)
    out_weight = noise(splits[8], (Q_HEADS * HEAD_DIM, D), (Q_HEADS * HEAD_DIM) ** -0.5, 0.1875, ((0, 4),))
    ffn_gain = jnp.clip(1.0 + 0.18 * jax.random.normal(splits[9], (D,), jnp.float32), 0.1, 1.9)
    routes_keys = jax.random.split(jax.random.fold_in(splits[10], 1), SEQS // SEQ_DEV)
    routes_turns = jax.random.permutation(jax.random.fold_in(splits[10], 3), SEQS // SEQ_DEV)
    routes = jax.vmap(lambda own, number: routed_block(jax.random.fold_in(splits[10], 2), own, number, SEQ_DEV, EXPERTS, TOP_K, CAP, 1))(routes_keys, routes_turns).reshape((SEQS, TOP_K))
    route_weights = jnp.clip(0.1 + 0.5 * jax.random.uniform(splits[11], (SEQS, TOP_K), jnp.float32) ** steps_of(splits[11], (SEQS, TOP_K), ((0, 64),), -0.2, 0.2), 0.1, 0.6)
    expert_gate = noise(splits[12], (EXPERTS, D, EXPERT_FF), D ** -0.5, 0.125, ((0, 64), (2, 4)))
    expert_up = noise(splits[13], (EXPERTS, D, EXPERT_FF), D ** -0.5, 0.125, ((0, 64), (2, 4)))
    expert_down = noise(splits[14], (EXPERTS, EXPERT_FF, D), EXPERT_FF ** -0.5, 0.1875, ((0, 64), (1, 4)))
    shared_gate = noise(splits[15], (D, SHARED_FF), D ** -0.5, 0.125, ((0, 64), (1, 4)))
    shared_up = noise(splits[16], (D, SHARED_FF), D ** -0.5, 0.125, ((0, 64), (1, 4)))
    shared_down = noise(splits[17], (SHARED_FF, D), SHARED_FF ** -0.5, 0.25, ((0, 4),))
    gate_vector = noise(splits[18], (D,), D ** -0.5, 0.125)
    return dict(tokens=tokens, lengths=lengths, cache=cache, attn_gain=attn_gain, query_weight=query_weight, key_weight=key_weight, value_weight=value_weight, stick_bias=stick_bias, out_weight=out_weight, ffn_gain=ffn_gain, routes=routes, route_weights=route_weights, expert_gate=expert_gate, expert_up=expert_up, expert_down=expert_down, shared_gate=shared_gate, shared_up=shared_up, shared_down=shared_down, gate_vector=gate_vector)


epsilon = 1e-06

def rms_scale(rows_in, gain_row):
    values_f = rows_in.astype(jnp.float32)
    return values_f * lax.rsqrt(lax.optimization_barrier(jnp.mean(values_f * values_f, axis=-1, keepdims=True)) + epsilon) * gain_row

def block_sum(left_rows, right_rows, blocks):
    row_count, inner = left_rows.shape
    part_width = inner // blocks
    left_view = left_rows.reshape(row_count, blocks, part_width).astype(jnp.float32)
    right_view = right_rows.reshape(blocks, part_width, right_rows.shape[1]).astype(jnp.float32)
    partials = jnp.einsum('nbf,bfd->bnd', left_view, right_view).astype(jnp.bfloat16)
    return lax.optimization_barrier(jnp.sum(partials.astype(jnp.float32), axis=0))

def reference(tokens, lengths, cache, attn_gain, query_weight, key_weight, value_weight, stick_bias, out_weight, ffn_gain, routes, route_weights, expert_gate, expert_up, expert_down, shared_gate, shared_up, shared_down, gate_vector):
    total_rows = tokens.shape[0]
    normed = rms_scale(tokens, attn_gain).astype(jnp.bfloat16)
    queries = jnp.dot(normed, query_weight, preferred_element_type=jnp.float32).astype(jnp.bfloat16)
    key_rows = jnp.dot(normed, key_weight, preferred_element_type=jnp.float32).astype(jnp.bfloat16)
    value_rows = jnp.dot(normed, value_weight, preferred_element_type=jnp.float32).astype(jnp.bfloat16)
    new_kv = jnp.stack([key_rows.reshape(total_rows, KV_HEADS, HEAD_DIM), value_rows.reshape(total_rows, KV_HEADS, HEAD_DIM)], axis=2)
    new_kv = new_kv.reshape(total_rows, 2 * KV_HEADS * HEAD_DIM)
    group_size = Q_HEADS // KV_HEADS
    grouped = queries.reshape(N_EP, SEQ_DEV, KV_HEADS, group_size, HEAD_DIM)
    cache_view = cache.reshape(N_EP, SEQ_DEV, CACHE, KV_HEADS, 2, HEAD_DIM)
    span_rows = lengths.reshape(N_EP, SEQ_DEV)
    offsets = stick_bias.astype(jnp.float32).reshape(1, KV_HEADS, group_size, 1)

    def attend(pieces):
        query_block, cache_block, span_block = pieces
        key_block = cache_block[:, :, :, 0, :].astype(jnp.float32)
        value_block = cache_block[:, :, :, 1, :].astype(jnp.float32)
        scores = jnp.einsum('nkgd,nckd->nkgc', query_block.astype(jnp.float32), key_block) * HEAD_DIM ** (-0.5)
        scores = scores + offsets
        positions = jnp.arange(CACHE, dtype=jnp.int32)
        usable = (positions[None, :] < span_block[:, None])[:, None, None, :]
        log_keep = jnp.where(usable, jax.nn.log_sigmoid(-scores), 0.0)
        behind = lax.cumsum(log_keep, axis=3, reverse=True) - log_keep
        stick_weights = jnp.where(usable, jnp.exp(jax.nn.log_sigmoid(scores) + behind), 0.0).astype(jnp.bfloat16)
        mixed = jnp.einsum('nkgc,nckd->nkgd', stick_weights.astype(jnp.float32), value_block)
        return mixed.astype(jnp.bfloat16)
    heads_out = lax.map(attend, (grouped, cache_view, span_rows)).reshape(total_rows, Q_HEADS * HEAD_DIM)
    residual = tokens.astype(jnp.float32) + block_sum(heads_out, out_weight, N_TP)
    normed_mix = rms_scale(residual, ffn_gain).astype(jnp.bfloat16)
    flat_routes = routes.reshape(-1)
    flat_weights = route_weights.reshape(-1).astype(jnp.float32)
    rows_most = N_EP * CAP

    def run_expert(expert_index):
        routed_here = flat_routes == expert_index
        ordering = jnp.argsort(jnp.where(routed_here, 0, 1).astype(jnp.int32), stable=True)[:rows_most]
        ordering = ordering.astype(jnp.int32)
        owners = (ordering // TOP_K).astype(jnp.int32)
        chosen = normed_mix[owners]
        gate_val = jnp.dot(chosen, expert_gate[expert_index], preferred_element_type=jnp.float32)
        up_val = jnp.dot(chosen, expert_up[expert_index], preferred_element_type=jnp.float32)
        hidden = (jax.nn.silu(gate_val) * up_val).astype(jnp.bfloat16)
        result = block_sum(hidden, expert_down[expert_index], N_TP).astype(jnp.bfloat16)
        route_scale = jnp.where(routed_here[ordering], flat_weights[ordering], 0.0)
        return (owners, result.astype(jnp.float32) * route_scale[:, None])
    owner_rows, contrib = lax.map(run_expert, jnp.arange(EXPERTS, dtype=jnp.int32))
    routed = jnp.zeros((total_rows, D), jnp.float32).at[owner_rows.reshape(-1)].add(contrib.reshape(-1, D))
    shared_gate_val = jnp.dot(normed_mix, shared_gate, preferred_element_type=jnp.float32)
    shared_up_val = jnp.dot(normed_mix, shared_up, preferred_element_type=jnp.float32)
    shared_hidden = (jax.nn.silu(shared_gate_val) * shared_up_val).astype(jnp.bfloat16)
    shared_out = block_sum(shared_hidden, shared_down, N_TP)
    mix_gate = jax.nn.sigmoid(jnp.dot(normed_mix, gate_vector, preferred_element_type=jnp.float32))
    layer_out = (residual + routed + mix_gate[:, None] * shared_out).astype(jnp.bfloat16)
    return (layer_out, new_kv)
```

```python
import jax
import jax.numpy as jnp
from jax import lax
from jax.experimental import pallas as pl
from jax.experimental.pallas import tpu as pltpu
from jax.sharding import PartitionSpec as P

HEAD_DIM = 64
EPS = 1e-06
CAP = 3
bf16 = jnp.bfloat16
f32 = jnp.float32

VM = pl.BlockSpec(memory_space=pltpu.VMEM)
SM = pl.BlockSpec(memory_space=pltpu.SMEM)
HBM = pl.BlockSpec(memory_space=pltpu.HBM)


def iota(shape, dim):
    return lax.broadcasted_iota(jnp.int32, shape, dim)


def dot(a, b, dims=((1,), (0,))):
    return lax.dot_general(a, b, (dims, ((), ())), preferred_element_type=f32)


def three_pieces(values):
    high = values.astype(bf16)
    rest = values - high.astype(f32)
    middle = rest.astype(bf16)
    low = (rest - middle.astype(f32)).astype(bf16)
    return high, middle, low


def call(kernel, outs, ins, in_specs=None, scratch=(), limit_mib=8):
    return pl.pallas_call(
        kernel,
        out_shape=tuple(jax.ShapeDtypeStruct(s, t) for s, t in outs),
        in_specs=in_specs or [VM] * len(ins),
        out_specs=tuple([VM] * len(outs)),
        scratch_shapes=list(scratch),
        compiler_params=pltpu.CompilerParams(vmem_limit_bytes=limit_mib * 1024 * 1024),
    )(*ins)


def attend_kernel(len_hbm, bias_hbm, tok_hbm, gain_hbm, cache_hbm, wq_hbm, wo_hbm,
                  part_ref, normed_ref,
                  len_ref, bias_ref, tok_ref, gain_ref, cache_v, wq_v, wo_v, s_v, sem_c, sem_w):
    rows = tok_ref.shape[0]
    span = cache_v.shape[1]
    heads = 4
    hr = rows * heads
    small = []
    for i, (src, dst) in enumerate(
        [(tok_hbm, tok_ref), (gain_hbm, gain_ref), (wq_hbm, wq_v), (wo_hbm, wo_v),
         (len_hbm, len_ref), (bias_hbm, bias_ref)]
    ):
        small.append(pltpu.make_async_copy(src, dst, sem_w.at[i]))
    tok_c, gain_c, wq_c, wo_c, len_c, bias_c = small
    tok_c.start()
    gain_c.start()
    wq_c.start()
    cache_c = []
    for n in range(rows):
        c = pltpu.make_async_copy(cache_hbm.at[n], cache_v.at[n], sem_c.at[n])
        c.start()
        cache_c.append(c)
    len_c.start()
    bias_c.start()
    wo_c.start()
    tok_c.wait()
    gain_c.wait()
    x = tok_ref[...].astype(f32)
    ms = jnp.mean(x * x, axis=-1, keepdims=True)
    normed = (x * lax.rsqrt(ms + EPS) * gain_ref[...]).astype(bf16)
    normed_ref[...] = normed
    expand = (iota((hr, rows), 0) // heads == iota((hr, rows), 1)).astype(bf16)
    lane = iota((hr, heads * HEAD_DIM), 1)
    row = iota((hr, heads * HEAD_DIM), 0)
    fold = ((iota((256, 128), 0) % HEAD_DIM) == iota((256, 128), 1)).astype(bf16)
    wq_c.wait()
    q = dot(normed, wq_v[...]).astype(bf16)
    qx = jnp.where(lane // HEAD_DIM == row % heads, dot(expand, q), 0.0).astype(bf16)
    qk = (dot(qx, fold) * (HEAD_DIM**-0.5)).astype(bf16)
    r16 = iota((16, span), 0) // heads
    for g in range(rows // 4):
        qg = qk[16 * g : 16 * g + 16, :]
        acc = None
        for i in range(4):
            n = 4 * g + i
            cache_c[n].wait()
            s = dot(qg, cache_v[n], ((1,), (1,)))
            acc = s if acc is None else jnp.where(r16 == i, s, acc)
        s_v[16 * g : 16 * g + 16, :] = acc
    rid = iota((hr, 128), 0)
    lens = jnp.zeros((hr, 128), jnp.int32)
    bias = jnp.zeros((hr, 128), f32)
    len_c.wait()
    bias_c.wait()
    for n in range(rows):
        lens = jnp.where(rid // heads == n, len_ref[n], lens)
    for h in range(heads):
        bias = jnp.where(rid % heads == h, bias_ref[h], bias)
    later = ((iota((128, 256), 0) > iota((128, 256), 1)) | (iota((128, 256), 1) >= 128)).astype(bf16)
    blocks = span // 128
    beyond = jnp.zeros((hr, 128), f32)
    weights = [None] * blocks
    for b in range(blocks - 1, -1, -1):
        z = s_v[:, b * 128 : (b + 1) * 128] + bias
        usable = (iota((hr, 128), 1) + b * 128) < lens
        soft = jnp.log1p(jnp.exp(-jnp.abs(z)))
        log_keep = jnp.where(usable, -(jnp.maximum(z, 0.0) + soft), 0.0)
        high, middle, low = three_pieces(log_keep)
        both = (dot(low, later) + dot(middle, later)) + dot(high, later)
        behind = both[:, :128] + beyond
        beyond = beyond + both[:, 128:]
        weights[b] = jnp.where(usable, jnp.exp(jnp.minimum(z, 0.0) - soft + behind), 0.0).astype(bf16)
    outs = []
    r16o = iota((16, 128), 0) // heads
    for g in range(rows // 4):
        pg = jnp.concatenate([w[16 * g : 16 * g + 16, :] for w in weights], axis=1)
        acc = None
        for i in range(4):
            o = dot(pg, cache_v[4 * g + i])
            acc = o if acc is None else jnp.where(r16o == i, o, acc)
        outs.append(acc)
    o = jnp.concatenate(outs, axis=0).astype(bf16)
    unfold = ((iota((128, 256), 0) - HEAD_DIM) == (iota((128, 256), 1) % HEAD_DIM)).astype(bf16)
    ox = jnp.where(lane // HEAD_DIM == row % heads, dot(o, unfold), 0.0).astype(bf16)
    collect = (iota((rows, hr), 1) // heads == iota((rows, hr), 0)).astype(bf16)
    heads_out = dot(collect, ox).astype(bf16)
    wo_c.wait()
    part_ref[...] = dot(heads_out, wo_v[...]).astype(bf16)


def attend(tokens, lengths, cache, gain, wq, bias, wo):
    rows, d = tokens.shape
    return call(
        attend_kernel, [((rows, d), bf16), ((rows, d), bf16)],
        (lengths, bias, tokens, gain.reshape(1, -1), cache, wq, wo),
        in_specs=[HBM] * 7,
        scratch=[
            pltpu.SMEM(lengths.shape, jnp.int32), pltpu.SMEM(bias.shape, f32),
            pltpu.VMEM(tokens.shape, bf16), pltpu.VMEM((1, d), f32),
            pltpu.VMEM(cache.shape, bf16), pltpu.VMEM(wq.shape, bf16), pltpu.VMEM(wo.shape, bf16),
            pltpu.VMEM((4 * rows, cache.shape[1]), f32),
            pltpu.SemaphoreType.DMA((rows,)), pltpu.SemaphoreType.DMA((6,)),
        ],
        limit_mib=16,
    )


def route_kernel(routes_ref, rw_ref, pick_ref, mix_ref):
    top, rows = routes_ref.shape
    experts = mix_ref.shape[1] // 8
    hits = jnp.zeros((experts, rows), f32)
    weight = jnp.zeros((experts, rows), f32)
    which = iota((experts, rows), 0)
    for j in range(top):
        same = which == routes_ref[j : j + 1, :]
        hits = jnp.where(same, 1.0, hits)
        weight = jnp.where(same, rw_ref[j : j + 1, :], weight)
    before = (iota((rows, rows), 0) < iota((rows, rows), 1)).astype(bf16)
    rank = dot(hits.astype(bf16), before)
    tile = (iota((rows, 8 * rows), 0) == iota((rows, 8 * rows), 1) % rows).astype(bf16)
    spread = (iota((8 * experts, experts), 0) // 8 == iota((8 * experts, experts), 1)).astype(bf16)
    here = (iota((8 * experts, 8 * rows), 0) % 8) == (iota((8 * experts, 8 * rows), 1) // rows)
    lane = iota((rows, 8 * experts), 1) % 8
    mixed = [jnp.zeros((rows, 8 * experts), f32) for _ in range(3)]
    for k in range(CAP):
        mine = jnp.where((hits > 0.5) & (rank == k), 1.0, 0.0)
        wide = dot(mine.astype(bf16), tile).astype(bf16)
        full = jnp.where(here, dot(spread, wide), 0.0)
        pick_ref[:, k * 8 * rows : (k + 1) * 8 * rows] = full.astype(bf16)
        for i, piece in enumerate(three_pieces(mine * weight)):
            part = dot(piece, spread, ((0,), (1,)))
            mixed[i] = jnp.where(lane // 2 == k, part, mixed[i])
    for h in range(2):
        for i in range(3):
            at = (h * 3 + i) * rows
            mix_ref[at : at + rows, :] = jnp.where(lane % 2 == h, mixed[i], 0.0).astype(bf16)


def mix_kernel(tok_ref, p0, p1, p2, p3, gain_ref, pick_ref, normed_ref, residual_ref, sent_ref):
    rows, d = tok_ref.shape
    wide = d // 8
    total = (p0[...].astype(f32) + p1[...].astype(f32)) + (p2[...].astype(f32) + p3[...].astype(f32))
    residual = tok_ref[...].astype(f32) + total
    residual_ref[...] = residual
    ms = jnp.mean(residual * residual, axis=-1, keepdims=True)
    normed = (residual * lax.rsqrt(ms + EPS) * gain_ref[...]).astype(bf16)
    normed_ref[...] = normed
    stacked = jnp.concatenate([normed[:, r * wide : (r + 1) * wide] for r in range(8)], axis=0)
    for k in range(CAP):
        pick = pick_ref[:, k * 8 * rows : (k + 1) * 8 * rows]
        sent_ref[:, k * wide : (k + 1) * wide] = dot(pick, stacked).astype(bf16)


def silu(v):
    return v / (1.0 + jnp.exp(-v))


def shared_kernel(ep_ref, normed_ref, gv_ref, b0, b1, b2, b3, b4, b5, b6, b7, hidden_ref, gate_ref):
    blocks = (b0, b1, b2, b3, b4, b5, b6, b7)
    rows, d = normed_ref.shape
    wide = d // 8
    ep = ep_ref[0]
    z = ep // 8
    y = (ep // 2) % 4
    c = ep % 2
    lane = iota((wide, wide), 1)
    there = ((y + 4 - lane // 64) % 4) * 64 + ((c + lane // 32) % 2) * 32 + lane % 32
    order = (iota((wide, wide), 0) == there).astype(bf16)
    cols = [normed_ref[:, pl.ds(pl.multiple_of(((z + 8 - j) % 8) * wide, wide), wide)] for j in range(8)]
    mine = dot(jnp.concatenate(cols, axis=0), order).astype(bf16)
    n = b0.shape[2]
    acc = jnp.zeros((rows, n), f32)
    for j in range(8):
        w = jnp.concatenate([b[j] for b in blocks], axis=0)
        acc = acc + dot(mine[j * rows : (j + 1) * rows, :], w)
    half = n // 2
    hidden = silu(acc[:, :half]) * acc[:, half:]
    hidden_ref[...] = hidden.astype(bf16)
    logit = jnp.sum(normed_ref[...].astype(f32) * gv_ref[...].astype(f32), axis=-1, keepdims=True)
    gate_ref[...] = jnp.broadcast_to(1.0 / (1.0 + jnp.exp(-logit)), gate_ref.shape)


def expert_kernel(arrived_ref, wg_ref, wu_ref, sh_ref, hidden_ref, x_v):
    n = arrived_ref.shape[0]
    peers = n // 8
    wide = arrived_ref.shape[1] // CAP
    a = iota((n, n), 0)
    b = iota((n, n), 1)
    order = ((b // 8 == a % peers) & (b % 8 == a // peers)).astype(bf16)
    sorted_rows = dot(order, arrived_ref[...]).astype(bf16)
    for r in range(8):
        for k in range(CAP):
            x_v[k * peers : (k + 1) * peers, r * wide : (r + 1) * wide] = sorted_rows[
                r * peers : (r + 1) * peers, k * wide : (k + 1) * wide
            ]
    x = x_v[...]
    gate = dot(x, wg_ref[0])
    up = dot(x, wu_ref[0])
    m = CAP * peers
    hidden_ref[:m, :] = (silu(gate) * up).astype(bf16)
    tail = hidden_ref.shape[0] - m
    sw = sh_ref.shape[1]
    hidden_ref[m:, :sw] = sh_ref[...]
    hidden_ref[m:, sw:] = jnp.zeros((tail, hidden_ref.shape[1] - sw), bf16)


def down_kernel(h0, h1, h2, h3, w0, w1, w2, w3, back_ref, shared_ref):
    hs = (h0, h1, h2, h3)
    ws = (w0, w1, w2, w3)
    n = back_ref.shape[0]
    peers = n // 8
    m = CAP * peers
    f = h0.shape[1]
    sw = w0.shape[0] - f
    acc = None
    sacc = None
    for h, w in zip(hs, ws):
        part = dot(h[:m, :], w[:f, :])
        acc = part if acc is None else acc + part
        part = dot(h[m:, :sw], w[f:, :])
        sacc = part if sacc is None else sacc + part
    shared_ref[...] = sacc
    out = acc.astype(bf16)
    half = out.shape[1] // 2
    pieces = [
        out[k * peers : (k + 1) * peers, h * half : (h + 1) * half] for k in range(CAP) for h in range(2)
    ]
    rhs = jnp.concatenate(pieces, axis=0)
    a = iota((n, 2 * m), 0)
    b = iota((n, 2 * m), 1)
    order = ((a % 8 == b // peers) & (a // 8 == b % peers)).astype(bf16)
    back_ref[...] = dot(order, rhs).astype(bf16)


def final_kernel(back_ref, mix_ref, residual_ref, shared_ref, gate_ref, out_ref):
    rows = out_ref.shape[0]
    half = out_ref.shape[1] // 2
    for h in range(2):
        r = dot(mix_ref[h * 3 * rows : (h + 1) * 3 * rows, :], back_ref[...])
        routed = (r[2 * rows :] + r[rows : 2 * rows]) + r[:rows]
        cols = slice(h * half, (h + 1) * half)
        total = residual_ref[:, cols] + routed + gate_ref[:, :1] * shared_ref[:, cols]
        out_ref[:, cols] = total.astype(bf16)


def around(k, size):
    return [(i, (i + k) % size) for i in range(size)]


def after(value, *deps):
    return lax.optimization_barrier((value, *deps))[0]


def shards(
    tokens, lengths, cache, attn_gain, query_weight, key_weight, value_weight, stick_bias, out_weight,
    ffn_gain, routes, route_weights, expert_gate, expert_up, expert_down, shared_gate, shared_up,
    shared_down, gate_vector,
):
    ntp = lax.axis_size("tp")
    nep = lax.axis_size("ep")
    rows, d = tokens.shape
    quarter = d // ntp
    part = lax.axis_index("tp")
    partial, normed = attend(tokens, lengths, cache, attn_gain, query_weight, stick_bias, out_weight)
    others = [lax.ppermute(partial, "tp", around(k, ntp)) for k in (2, 1, 3)]

    n_pick = 8 * nep
    pick, mix = call(
        route_kernel, [((n_pick, CAP * 8 * rows), bf16), ((6 * rows, n_pick), bf16)],
        (after(routes.T, partial), route_weights.T),
    )
    normed_mix, residual_full, sent = call(
        mix_kernel, [((rows, d), bf16), ((rows, d), f32), ((n_pick, CAP * d // 8), bf16)],
        (tokens, partial, *others, ffn_gain.reshape(1, -1), pick),
    )
    arrived = lax.all_to_all(sent.reshape(nep, 8, -1), "ep", 0, 0, tiled=True)
    arrived = arrived.reshape(n_pick, -1)

    joined = after(jnp.concatenate([shared_gate, shared_up], axis=1), sent)

    def shift(value, dz, dy, dc):
        perm = []
        for i in range(nep):
            z, y, c = i // 8, i // 2 % 4, i % 2
            perm.append((i, (z + dz) % (nep // 8) * 8 + (y + dy) % 4 * 2 + (c + dc) % 2))
        return lax.ppermute(value, "ep", perm)

    column = jnp.stack([joined] + [shift(joined, k, 0, 0) for k in range(1, nep // 8)])
    planes = [column] + [shift(column, 0, k, 0) for k in range(1, 4)]
    blocks = []
    for block in planes:
        blocks += [block, shift(block, 0, 0, 1)]
    down_all = after(jnp.concatenate([expert_down[0], shared_down], axis=0), sent)
    downs = []
    for k in range(ntp):
        cut = lax.dynamic_slice_in_dim(down_all, ((part + k) % ntp) * quarter, quarter, 1)
        downs.append(cut if k == 0 else lax.ppermute(cut, "tp", around(k, ntp)))
    shared_hidden, mix_gate = call(
        shared_kernel, [((rows, shared_gate.shape[1]), bf16), ((rows, 128), f32)],
        (lax.axis_index("ep").reshape(1), normed_mix, gate_vector.reshape(1, -1), *blocks),
        in_specs=[SM] + [VM] * 10,
    )
    m = CAP * nep
    (hidden,) = call(
        expert_kernel, [((m + rows, expert_gate.shape[2]), bf16)],
        (arrived, expert_gate, expert_up, shared_hidden), scratch=[pltpu.VMEM((m, d), bf16)],
    )
    hiddens = [hidden] + [lax.ppermute(hidden, "tp", around(k, ntp)) for k in range(1, ntp)]
    back, shared_out = call(down_kernel, [((n_pick, quarter // 2), bf16), ((rows, quarter), f32)], (*hiddens, *downs))
    returned = lax.all_to_all(back.reshape(nep, 8, -1), "ep", 0, 0, tiled=True).reshape(n_pick, -1)
    late = after(normed, back)
    residual = lax.dynamic_slice_in_dim(residual_full, part * quarter, quarter, 1)
    local_heads = key_weight.shape[1] // HEAD_DIM
    key_rows = jnp.dot(late, key_weight, preferred_element_type=f32).astype(bf16)
    value_rows = jnp.dot(late, value_weight, preferred_element_type=f32).astype(bf16)
    new_kv = jnp.stack(
        [key_rows.reshape(rows, local_heads, HEAD_DIM), value_rows.reshape(rows, local_heads, HEAD_DIM)], axis=2
    ).reshape(rows, -1)
    (layer_out,) = call(final_kernel, [((rows, quarter), bf16)], (returned, mix, residual, shared_out, mix_gate))
    return (layer_out, new_kv)


def solution(mesh):
    placed = (
        P("ep", None), P("ep"), P("ep", None, "tp"), P(), P(None, "tp"), P(None, "tp"), P(None, "tp"),
        P("tp"), P("tp", None), P(), P("ep", None), P("ep", None), P("ep", None, "tp"),
        P("ep", None, "tp"), P("ep", "tp", None), P("ep", "tp"), P("ep", "tp"), P("tp", None), P(),
    )

    return jax.shard_map(shards, mesh=mesh, in_specs=placed, out_specs=(P("ep", "tp"), P("ep", "tp")), check_vma=False)
```

```python
import jax
import jax.numpy as jnp
from jax import lax
from jax.experimental import pallas as pl
from jax.experimental.pallas import tpu as pltpu
from jax.sharding import PartitionSpec as P

HEAD_DIM = 64
EPS = 1e-06
CAP = 3
bf16 = jnp.bfloat16
f32 = jnp.float32

VM = pl.BlockSpec(memory_space=pltpu.VMEM)
SM = pl.BlockSpec(memory_space=pltpu.SMEM)
HBM = pl.BlockSpec(memory_space=pltpu.HBM)


def iota(shape, dim):
    return lax.broadcasted_iota(jnp.int32, shape, dim)


def dot(a, b, dims=((1,), (0,))):
    return lax.dot_general(a, b, (dims, ((), ())), preferred_element_type=f32)


def three_pieces(values):
    high = values.astype(bf16)
    rest = values - high.astype(f32)
    middle = rest.astype(bf16)
    low = (rest - middle.astype(f32)).astype(bf16)
    return high, middle, low


def hbm(value):
    return pltpu.with_memory_space_constraint(value, pltpu.HBM)


def call(kernel, outs, ins, in_specs=None, out_specs=None, scratch=(), limit_mib=8):
    in_specs = in_specs or [VM] * len(ins)
    out_specs = out_specs or [VM] * len(outs)
    ins = [hbm(x) if spec is HBM else x for x, spec in zip(ins, in_specs)]
    shapes = [
        pltpu.HBM(s, t) if spec is HBM else jax.ShapeDtypeStruct(s, t) for (s, t), spec in zip(outs, out_specs)
    ]
    return pl.pallas_call(
        kernel,
        out_shape=tuple(shapes),
        in_specs=in_specs,
        out_specs=tuple(out_specs),
        scratch_shapes=list(scratch),
        compiler_params=pltpu.CompilerParams(vmem_limit_bytes=limit_mib * 1024 * 1024),
    )(*ins)


def copy_all(pairs, sems, first=0):
    copies = [pltpu.make_async_copy(src, dst, sems.at[first + i]) for i, (src, dst) in enumerate(pairs)]
    for c in copies:
        c.start()
    return copies


def attend_kernel(len_hbm, bias_hbm, tok_hbm, gain_hbm, cache_hbm, wq_hbm, wo_hbm, sg_hbm, su_hbm,
                  part_ref, joined_hbm,
                  len_ref, bias_ref, tok_ref, gain_ref, cache_v, wq_v, wo_v, s_v, joined_v, sem_c, sem_w, sem_j):
    rows = tok_ref.shape[0]
    span = cache_v.shape[1]
    heads = 4
    hr = rows * heads
    small = []
    for i, (src, dst) in enumerate(
        [(tok_hbm, tok_ref), (gain_hbm, gain_ref), (wq_hbm, wq_v), (wo_hbm, wo_v),
         (len_hbm, len_ref), (bias_hbm, bias_ref)]
    ):
        small.append(pltpu.make_async_copy(src, dst, sem_w.at[i]))
    tok_c, gain_c, wq_c, wo_c, len_c, bias_c = small
    tok_c.start()
    gain_c.start()
    wq_c.start()
    cache_c = []
    for n in range(rows):
        c = pltpu.make_async_copy(cache_hbm.at[n], cache_v.at[n], sem_c.at[n])
        c.start()
        cache_c.append(c)
    len_c.start()
    bias_c.start()
    wo_c.start()
    width = sg_hbm.shape[1]
    for c in copy_all([(sg_hbm, joined_v.at[:, :width]), (su_hbm, joined_v.at[:, width:])], sem_j, 8):
        small.append(c)
    tok_c.wait()
    gain_c.wait()
    x = tok_ref[...].astype(f32)
    ms = jnp.mean(x * x, axis=-1, keepdims=True)
    normed = (x * lax.rsqrt(ms + EPS) * gain_ref[...]).astype(bf16)
    expand = (iota((hr, rows), 0) // heads == iota((hr, rows), 1)).astype(bf16)
    lane = iota((hr, heads * HEAD_DIM), 1)
    row = iota((hr, heads * HEAD_DIM), 0)
    fold = ((iota((256, 128), 0) % HEAD_DIM) == iota((256, 128), 1)).astype(bf16)
    wq_c.wait()
    q = dot(normed, wq_v[...]).astype(bf16)
    qx = jnp.where(lane // HEAD_DIM == row % heads, dot(expand, q), 0.0).astype(bf16)
    qk = (dot(qx, fold) * (HEAD_DIM**-0.5)).astype(bf16)
    wide_q = jnp.concatenate([qk] * 4, axis=1)
    own_seq = iota(wide_q.shape, 1) // 128 == (iota(wide_q.shape, 0) // heads) % 4
    wide_q = jnp.where(own_seq, wide_q.astype(f32), 0.0).astype(bf16)
    for g in range(rows // 4):
        for n in range(4 * g, 4 * g + 4):
            cache_c[n].wait()
        keys = jnp.concatenate([cache_v[n] for n in range(4 * g, 4 * g + 4)], axis=1)
        s_v[16 * g : 16 * g + 16, :] = dot(wide_q[16 * g : 16 * g + 16, :], keys, ((1,), (1,)))
    for c in small[6:]:
        c.wait()
    sends = copy_all([(joined_v, joined_hbm.at[j]) for j in range(joined_hbm.shape[0])], sem_j)
    rid = iota((hr, 128), 0)
    lens = jnp.zeros((hr, 128), jnp.int32)
    bias = jnp.zeros((hr, 128), f32)
    len_c.wait()
    bias_c.wait()
    for n in range(rows):
        lens = jnp.where(rid // heads == n, len_ref[n], lens)
    for h in range(heads):
        bias = jnp.where(rid % heads == h, bias_ref[h], bias)
    later = ((iota((128, 256), 0) > iota((128, 256), 1)) | (iota((128, 256), 1) >= 128)).astype(bf16)
    blocks = span // 128
    usable, own, pieces = [], [], []
    for b in range(blocks):
        z = s_v[:, b * 128 : (b + 1) * 128] + bias
        ok = (iota((hr, 128), 1) + b * 128) < lens
        soft = jnp.log1p(jnp.exp(-jnp.abs(z)))
        usable.append(ok)
        own.append(jnp.minimum(z, 0.0) - soft)
        pieces.append(three_pieces(jnp.where(ok, -(jnp.maximum(z, 0.0) + soft), 0.0)))
    high, middle, low = [jnp.concatenate([p[i] for p in pieces], axis=0) for i in range(3)]
    both = (dot(low, later) + dot(middle, later)) + dot(high, later)
    beyond = jnp.zeros((hr, 128), f32)
    weights = [None] * blocks
    for b in range(blocks - 1, -1, -1):
        mine = both[b * hr : (b + 1) * hr, :]
        behind = mine[:, :128] + beyond
        beyond = beyond + mine[:, 128:]
        weights[b] = jnp.where(usable[b], jnp.exp(own[b] + behind), 0.0).astype(bf16)
    outs = []
    r16o = iota((16, 128), 0) // heads
    for g in range(rows // 4):
        pg = jnp.concatenate([w[16 * g : 16 * g + 16, :] for w in weights], axis=1)
        acc = None
        for i in range(4):
            o = dot(pg, cache_v[4 * g + i])
            acc = o if acc is None else jnp.where(r16o == i, o, acc)
        outs.append(acc)
    o = jnp.concatenate(outs, axis=0).astype(bf16)
    unfold = ((iota((128, 256), 0) - HEAD_DIM) == (iota((128, 256), 1) % HEAD_DIM)).astype(bf16)
    ox = jnp.where(lane // HEAD_DIM == row % heads, dot(o, unfold), 0.0).astype(bf16)
    collect = (iota((rows, hr), 1) // heads == iota((rows, hr), 0)).astype(bf16)
    heads_out = dot(collect, ox).astype(bf16)
    wo_c.wait()
    part_ref[...] = dot(heads_out, wo_v[...]).astype(bf16)
    for c in sends:
        c.wait()


def attend(tokens, lengths, cache, gain, wq, bias, wo, shared_gate, shared_up):
    rows, d = tokens.shape
    joined = (shared_gate.shape[0], 2 * shared_gate.shape[1])
    return call(
        attend_kernel, [((rows, d), bf16), ((8, *joined), bf16)],
        (lengths, bias, tokens, gain.reshape(1, -1), cache, wq, wo, shared_gate, shared_up),
        in_specs=[HBM] * 9, out_specs=[VM, HBM],
        scratch=[
            pltpu.SMEM(lengths.shape, jnp.int32), pltpu.SMEM(bias.shape, f32),
            pltpu.VMEM(tokens.shape, bf16), pltpu.VMEM((1, d), f32),
            pltpu.VMEM(cache.shape, bf16), pltpu.VMEM(wq.shape, bf16), pltpu.VMEM(wo.shape, bf16),
            pltpu.VMEM((4 * rows, cache.shape[1]), f32),
            pltpu.VMEM(joined, bf16),
            pltpu.SemaphoreType.DMA((rows,)), pltpu.SemaphoreType.DMA((6,)), pltpu.SemaphoreType.DMA((10,)),
        ],
        limit_mib=16,
    )


def slots_of(routes_ref, rw_ref):
    top, rows = routes_ref.shape
    experts = 64
    hits = jnp.zeros((experts, rows), f32)
    weight = jnp.zeros((experts, rows), f32)
    which = iota((experts, rows), 0)
    for j in range(top):
        same = which == routes_ref[j : j + 1, :]
        hits = jnp.where(same, 1.0, hits)
        if rw_ref is not None:
            weight = jnp.where(same, rw_ref[j : j + 1, :], weight)
    before = (iota((rows, rows), 0) < iota((rows, rows), 1)).astype(bf16)
    rank = dot(hits.astype(bf16), before)
    slots = [jnp.where((hits > 0.5) & (rank == k), 1.0, 0.0) for k in range(CAP)]
    spread = (iota((8 * experts, experts), 0) // 8 == iota((8 * experts, experts), 1)).astype(bf16)
    return slots, weight, spread


def pick_kernel(routes_ref, pick_ref):
    rows = routes_ref.shape[1]
    slots, _, spread = slots_of(routes_ref, None)
    n = spread.shape[0]
    tile = (iota((rows, 8 * rows), 0) == iota((rows, 8 * rows), 1) % rows).astype(bf16)
    here = (iota((n, 8 * rows), 0) % 8) == (iota((n, 8 * rows), 1) // rows)
    for k in range(CAP):
        wide = dot(slots[k].astype(bf16), tile).astype(bf16)
        full = jnp.where(here, dot(spread, wide), 0.0)
        pick_ref[:, k * 8 * rows : (k + 1) * 8 * rows] = full.astype(bf16)


def mix_kernel(part_ref, tok_ref, p0, p1, p2, p3, gain_ref, pick_ref, normed_hbm, residual_hbm, sent_hbm,
               normed_v, residual_v, sent_v, sems):
    rows, d = tok_ref.shape
    wide = d // 8
    quarter = residual_hbm.shape[1]
    total = (p0[...].astype(f32) + p1[...].astype(f32)) + (p2[...].astype(f32) + p3[...].astype(f32))
    residual = tok_ref[...].astype(f32) + total
    residual_v[...] = residual
    ms = jnp.mean(residual * residual, axis=-1, keepdims=True)
    normed = (residual * lax.rsqrt(ms + EPS) * gain_ref[...]).astype(bf16)
    normed_v[...] = normed
    mine = pl.ds(pl.multiple_of(part_ref[0] * quarter, quarter), quarter)
    copies = copy_all([(normed_v, normed_hbm), (residual_v.at[:, mine], residual_hbm)], sems)
    stacked = jnp.concatenate([normed[:, r * wide : (r + 1) * wide] for r in range(8)], axis=0)
    for k in range(CAP):
        pick = pick_ref[:, k * 8 * rows : (k + 1) * 8 * rows]
        cols = slice(k * wide, (k + 1) * wide)
        sent_v[:, cols] = dot(pick, stacked).astype(bf16)
        copies += copy_all([(sent_v.at[:, cols], sent_hbm.at[:, cols])], sems, 2 + k)
    for c in copies:
        c.wait()


def cut_kernel(part_ref, down_hbm, shared_hbm, o0, o1, o2, o3, all_v, sems):
    outs = (o0, o1, o2, o3)
    quarter = o0.shape[1]
    f = down_hbm.shape[1]
    first = copy_all([(down_hbm.at[0], all_v.at[:f, :]), (shared_hbm, all_v.at[f:, :])], sems, 4)
    for c in first:
        c.wait()
    pairs = []
    for k in (1, 3, 2, 0):
        cols = pl.ds(pl.multiple_of(((part_ref[0] + k) % 4) * quarter, quarter), quarter)
        pairs.append((all_v.at[:, cols], outs[k]))
    for c in copy_all(pairs, sems):
        c.wait()


def silu(v):
    return v / (1.0 + jnp.exp(-v))


def shared_kernel(ep_ref, normed_ref, b0, b1, b2, b3, b4, b5, b6, b7, hidden_ref):
    blocks = (b0, b1, b2, b3, b4, b5, b6, b7)
    rows, d = normed_ref.shape
    wide = d // 8
    ep = ep_ref[0]
    y = (ep // 2) % 4
    c = ep % 2
    lane = iota((wide, wide), 1)
    there = ((y + 4 - lane // 64) % 4) * 64 + ((c + lane // 32) % 2) * 32 + lane % 32
    order = (iota((wide, wide), 0) == there).astype(bf16)
    cols = [normed_ref[:, j * wide : (j + 1) * wide] for j in range(8)]
    mine = dot(jnp.concatenate(cols, axis=0), order).astype(bf16)
    n = b0.shape[2]
    acc = jnp.zeros((rows, n), f32)
    for j in range(8):
        w = jnp.concatenate([b[j] for b in blocks], axis=0)
        acc = acc + dot(mine[j * rows : (j + 1) * rows, :], w)
    half = n // 2
    hidden = silu(acc[:, :half]) * acc[:, half:]
    hidden_ref[...] = hidden.astype(bf16)


def expert_kernel(arrived_ref, wg_ref, wu_ref, sh_ref, hidden_ref, x_v):
    n = arrived_ref.shape[0]
    peers = n // 8
    wide = arrived_ref.shape[1] // CAP
    a = iota((n, n), 0)
    b = iota((n, n), 1)
    order = ((b // 8 == a % peers) & (b % 8 == a // peers)).astype(bf16)
    sorted_rows = dot(order, arrived_ref[...]).astype(bf16)
    for r in range(8):
        for k in range(CAP):
            x_v[k * peers : (k + 1) * peers, r * wide : (r + 1) * wide] = sorted_rows[
                r * peers : (r + 1) * peers, k * wide : (k + 1) * wide
            ]
    x = x_v[...]
    gate = dot(x, wg_ref[0])
    up = dot(x, wu_ref[0])
    m = CAP * peers
    hidden_ref[:m, :] = (silu(gate) * up).astype(bf16)
    hidden_ref[m:, : sh_ref.shape[1]] = sh_ref[...]
    hidden_ref[m:, sh_ref.shape[1] :] = jnp.zeros((sh_ref.shape[0], hidden_ref.shape[1] - sh_ref.shape[1]), bf16)


def down_kernel(h0, h1, h2, h3, w0, w1, w2, w3, back_ref, w_v, sems):
    n = back_ref.shape[0]
    peers = n // 8
    f = h0.shape[1]
    m = CAP * peers
    copies = copy_all([(w.at[:f, :], w_v.at[k]) for k, w in enumerate((w0, w1, w2, w3))], sems)
    a = iota((n, 2 * m), 0)
    b = iota((n, 2 * m), 1)
    order = ((a % 8 == b // peers) & (a // 8 == b % peers)).astype(bf16)
    acc = None
    for k, h in enumerate((h0, h1, h2, h3)):
        copies[k].wait()
        part = dot(h[:m, :], w_v[k])
        acc = part if acc is None else acc + part
    out = acc.astype(bf16)
    half = out.shape[1] // 2
    pieces = [
        out[k * peers : (k + 1) * peers, h * half : (h + 1) * half] for k in range(CAP) for h in range(2)
    ]
    rhs = jnp.concatenate(pieces, axis=0)
    back_ref[...] = dot(order, rhs).astype(bf16)


def side_kernel(routes_ref, rw_ref, tok_hbm, gain_ref, kw_hbm, vw_hbm, mixed_hbm, gv_ref,
                mix_ref, kv_ref, gate_ref, tok_ref, both_ref, mixed_ref, sems):
    rows = tok_ref.shape[0]
    n = kw_hbm.shape[0]
    copies = copy_all([(tok_hbm, tok_ref), (kw_hbm, both_ref.at[:n, :]), (vw_hbm, both_ref.at[n:, :]),
                       (mixed_hbm, mixed_ref)], sems)
    for c in copies:
        c.wait()
    x = tok_ref[...].astype(f32)
    ms = jnp.mean(x * x, axis=-1, keepdims=True)
    normed = (x * lax.rsqrt(ms + EPS) * gain_ref[...]).astype(bf16)
    kv_ref[...] = dot(normed, both_ref[...], ((1,), (1,))).astype(bf16)
    slots, weight, spread = slots_of(routes_ref, rw_ref)
    lane = iota((rows, spread.shape[0]), 1) % 8
    mixed = [jnp.zeros(lane.shape, f32) for _ in range(3)]
    for k in range(CAP):
        for i, piece in enumerate(three_pieces(slots[k] * weight)):
            mixed[i] = jnp.where(lane // 2 == k, dot(piece, spread, ((0,), (1,))), mixed[i])
    for h in range(2):
        for i in range(3):
            row = (h * 3 + i) * rows
            mix_ref[row : row + rows, :] = jnp.where(lane % 2 == h, mixed[i], 0.0).astype(bf16)
    total = jnp.zeros((rows, 128), f32)
    for j in range(gv_ref.shape[0]):
        total = total + mixed_ref[:, j * 128 : (j + 1) * 128].astype(f32) * gv_ref[j : j + 1, :].astype(f32)
    logit = jnp.sum(total, axis=-1, keepdims=True)
    gate_ref[...] = jnp.broadcast_to(1.0 / (1.0 + jnp.exp(-logit)), gate_ref.shape)


def base_kernel(residual_hbm, gate_ref, s0, s1, s2, s3, w0, w1, w2, w3, base_ref, residual_v, w_v, sems):
    at = w0.shape[0] - w_v.shape[1]
    copies = copy_all([(w.at[at:, :], w_v.at[k]) for k, w in enumerate((w0, w1, w2, w3))], sems)
    copies += copy_all([(residual_hbm, residual_v)], sems, 4)
    acc = None
    for k, h in enumerate((s0, s1, s2, s3)):
        copies[k].wait()
        part = dot(h[h.shape[0] - base_ref.shape[0] :, : w_v.shape[1]], w_v[k])
        acc = part if acc is None else acc + part
    copies[4].wait()
    base_ref[...] = residual_v[...] + gate_ref[:, :1] * acc


def final_kernel(back_ref, mix_ref, base_ref, out_ref):
    rows = out_ref.shape[0]
    half = out_ref.shape[1] // 2
    for h in range(2):
        r = dot(mix_ref[h * 3 * rows : (h + 1) * 3 * rows, :], back_ref[...])
        routed = (r[2 * rows :] + r[rows : 2 * rows]) + r[:rows]
        cols = slice(h * half, (h + 1) * half)
        out_ref[:, cols] = (base_ref[:, cols] + routed).astype(bf16)


def around(k, size):
    return [(i, (i + k) % size) for i in range(size)]


def after(value, *deps):
    return lax.optimization_barrier((value, *deps))[0]


def shards(
    tokens, lengths, cache, attn_gain, query_weight, key_weight, value_weight, stick_bias, out_weight,
    ffn_gain, routes, route_weights, expert_gate, expert_up, expert_down, shared_gate, shared_up,
    shared_down, gate_vector,
):
    ntp = lax.axis_size("tp")
    nep = lax.axis_size("ep")
    rows, d = tokens.shape
    quarter = d // ntp
    part = lax.axis_index("tp").reshape(1)
    n_pick = 8 * nep

    def shift(value, dz, dy, dc):
        perm = []
        for i in range(nep):
            z, y, c = i // 8, i // 2 % 4, i % 2
            perm.append((i, (z + dz) % (nep // 8) * 8 + (y + dy) % 4 * 2 + (c + dc) % 2))
        return lax.ppermute(value, "ep", perm)

    partial, copies = attend(
        tokens, lengths, cache, attn_gain, query_weight, stick_bias, out_weight, shared_gate, shared_up
    )
    groups = [[z * 8 + r for z in range(nep // 8)] for r in range(8)]
    others = [lax.ppermute(partial, "tp", around(k, ntp)) for k in (2, 1, 3)]
    column = lax.all_to_all(copies, "ep", 0, 0, axis_index_groups=groups, tiled=True)
    (pick,) = call(pick_kernel, [((n_pick, CAP * 8 * rows), bf16)], (after(routes.T, partial),))
    normed_mix, residual, sent = call(
        mix_kernel, [((rows, d), bf16), ((rows, quarter), f32), ((n_pick, CAP * d // 8), bf16)],
        (part, tokens, partial, *others, ffn_gain.reshape(1, -1), pick),
        in_specs=[SM] + [VM] * 7, out_specs=[HBM] * 3,
        scratch=[pltpu.VMEM((rows, d), bf16), pltpu.VMEM((rows, d), f32),
                 pltpu.VMEM((n_pick, CAP * d // 8), bf16), pltpu.SemaphoreType.DMA((5,))],
    )
    arrived = lax.all_to_all(sent.reshape(nep, 8, -1), "ep", 0, 0, tiled=True)
    arrived = arrived.reshape(n_pick, -1)
    column = after(column, sent)
    planes = [column] + [shift(column, 0, k, 0) for k in range(1, 4)]
    blocks = []
    for block in planes:
        blocks += [block, shift(block, 0, 0, 1)]
    f = expert_down.shape[1] + shared_down.shape[0]
    cuts = call(
        cut_kernel, [((f, quarter), bf16)] * 4, (part, after(expert_down, sent), shared_down),
        in_specs=[SM, HBM, HBM], out_specs=[HBM] * 4,
        scratch=[pltpu.VMEM((f, d), bf16), pltpu.SemaphoreType.DMA((6,))],
    )
    downs = [cuts[0]] + [lax.ppermute(cuts[k], "tp", around(k, ntp)) for k in range(1, ntp)]
    mix, new_kv, mix_gate = call(
        side_kernel,
        [((6 * rows, n_pick), bf16), ((rows, 2 * HEAD_DIM), bf16), ((rows, 128), f32)],
        (routes.T, route_weights.T, after(tokens, sent), attn_gain.reshape(1, -1), key_weight.T, value_weight.T,
         normed_mix, gate_vector.reshape(-1, 128)),
        in_specs=[VM, VM, HBM, VM, HBM, HBM, HBM, VM],
        scratch=[pltpu.VMEM((rows, d), bf16), pltpu.VMEM((2 * HEAD_DIM, d), bf16), pltpu.VMEM((rows, d), bf16),
                 pltpu.SemaphoreType.DMA((4,))],
    )
    (shared_hidden,) = call(
        shared_kernel, [((rows, shared_gate.shape[1]), bf16)],
        (lax.axis_index("ep").reshape(1), normed_mix, *blocks), in_specs=[SM] + [VM] * 9,
    )
    m = CAP * nep
    (hidden,) = call(
        expert_kernel, [((m + rows, expert_gate.shape[2]), bf16)],
        (arrived, expert_gate, expert_up, shared_hidden), scratch=[pltpu.VMEM((m, d), bf16)],
    )
    hiddens = [hidden] + [lax.ppermute(hidden, "tp", around(k, ntp)) for k in range(1, ntp)]
    (back,) = call(
        down_kernel, [((n_pick, quarter // 2), bf16)], (*hiddens, *downs), in_specs=[VM] * 4 + [HBM] * 4,
        scratch=[pltpu.VMEM((ntp, expert_down.shape[1], quarter), bf16), pltpu.SemaphoreType.DMA((4,))],
    )
    returned = lax.all_to_all(back.reshape(nep, 8, -1), "ep", 0, 0, tiled=True)
    returned = returned.reshape(n_pick, -1)
    (base,) = call(
        base_kernel, [((rows, quarter), f32)], (after(residual, back), mix_gate, *hiddens, *downs),
        in_specs=[HBM] + [VM] * 5 + [HBM] * 4,
        scratch=[pltpu.VMEM((rows, quarter), f32), pltpu.VMEM((ntp, shared_down.shape[0], quarter), bf16),
                 pltpu.SemaphoreType.DMA((5,))],
    )
    (layer_out,) = call(final_kernel, [((rows, quarter), bf16)], (returned, mix, base))
    return (layer_out, new_kv)


def solution(mesh):
    placed = (
        P("ep", None), P("ep"), P("ep", None, "tp"), P(), P(None, "tp"), P(None, "tp"), P(None, "tp"),
        P("tp"), P("tp", None), P(), P("ep", None), P("ep", None), P("ep", None, "tp"),
        P("ep", None, "tp"), P("ep", "tp", None), P("ep", "tp"), P("ep", "tp"), P("tp", None), P(),
    )

    return jax.shard_map(shards, mesh=mesh, in_specs=placed, out_specs=(P("ep", "tp"), P("ep", "tp")), check_vma=False)
```

```python
import jax
import jax.numpy as jnp
from jax import lax
from jax.experimental import pallas as pl
from jax.experimental.pallas import tpu as pltpu
from jax.sharding import PartitionSpec as P

HEAD_DIM = 64
EPS = 1e-06
CAP = 3
Z_ORDER = (0, -1, 1, -3, -4, -2, 3, 2)
bf16 = jnp.bfloat16
f32 = jnp.float32

VM = pl.BlockSpec(memory_space=pltpu.VMEM)
SM = pl.BlockSpec(memory_space=pltpu.SMEM)
HBM = pl.BlockSpec(memory_space=pltpu.HBM)


def iota(shape, dim):
    return lax.broadcasted_iota(jnp.int32, shape, dim)


def dot(a, b, dims=((1,), (0,))):
    return lax.dot_general(a, b, (dims, ((), ())), preferred_element_type=f32)


def three_pieces(values):
    high = values.astype(bf16)
    rest = values - high.astype(f32)
    middle = rest.astype(bf16)
    low = (rest - middle.astype(f32)).astype(bf16)
    return high, middle, low


def hbm(value):
    return pltpu.with_memory_space_constraint(value, pltpu.HBM)


def call(kernel, outs, ins, in_specs=None, out_specs=None, scratch=(), limit_mib=8):
    in_specs = in_specs or [VM] * len(ins)
    out_specs = out_specs or [VM] * len(outs)
    ins = [hbm(x) if spec is HBM else x for x, spec in zip(ins, in_specs)]
    shapes = [
        pltpu.HBM(s, t) if spec is HBM else jax.ShapeDtypeStruct(s, t) for (s, t), spec in zip(outs, out_specs)
    ]
    return pl.pallas_call(
        kernel,
        out_shape=tuple(shapes),
        in_specs=in_specs,
        out_specs=tuple(out_specs),
        scratch_shapes=list(scratch),
        compiler_params=pltpu.CompilerParams(vmem_limit_bytes=limit_mib * 1024 * 1024),
    )(*ins)


def copy_all(pairs, sems, first=0):
    copies = [pltpu.make_async_copy(src, dst, sems.at[first + i]) for i, (src, dst) in enumerate(pairs)]
    for c in copies:
        c.start()
    return copies


def attend_kernel(len_hbm, bias_hbm, tok_hbm, gain_hbm, cache_hbm, wq_hbm, wo_hbm, routes_hbm, sg_hbm, su_hbm,
                  part_ref, pick_ref, joined_ref,
                  len_ref, bias_ref, tok_ref, gain_ref, cache_v, wq_v, wo_v, s_v, routes_v, sem_c, sem_w):
    rows = tok_ref.shape[0]
    span = cache_v.shape[1]
    heads = 4
    hr = rows * heads
    small = []
    for i, (src, dst) in enumerate(
        [(tok_hbm, tok_ref), (gain_hbm, gain_ref), (wq_hbm, wq_v), (wo_hbm, wo_v),
         (len_hbm, len_ref), (bias_hbm, bias_ref)]
    ):
        small.append(pltpu.make_async_copy(src, dst, sem_w.at[i]))
    tok_c, gain_c, wq_c, wo_c, len_c, bias_c = small
    routes_c = pltpu.make_async_copy(routes_hbm, routes_v, sem_w.at[6])
    routes_c.start()
    tok_c.start()
    gain_c.start()
    wq_c.start()
    cache_c = []
    for n in range(rows):
        c = pltpu.make_async_copy(cache_hbm.at[n], cache_v.at[n], sem_c.at[n])
        c.start()
        cache_c.append(c)
    len_c.start()
    bias_c.start()
    wo_c.start()
    half = sg_hbm.shape[1]
    joins = copy_all([(sg_hbm, joined_ref.at[0, :, :half]), (su_hbm, joined_ref.at[0, :, half:])], sem_w, 7)
    routes_c.wait()
    make_pick(routes_v, pick_ref)
    tok_c.wait()
    gain_c.wait()
    x = tok_ref[...].astype(f32)
    ms = jnp.mean(x * x, axis=-1, keepdims=True)
    normed = (x * lax.rsqrt(ms + EPS) * gain_ref[...]).astype(bf16)
    expand = (iota((hr, rows), 0) // heads == iota((hr, rows), 1)).astype(bf16)
    lane = iota((hr, heads * HEAD_DIM), 1)
    row = iota((hr, heads * HEAD_DIM), 0)
    fold = ((iota((256, 128), 0) % HEAD_DIM) == iota((256, 128), 1)).astype(bf16)
    wq_c.wait()
    q = dot(normed, wq_v[...]).astype(bf16)
    qx = jnp.where(lane // HEAD_DIM == row % heads, dot(expand, q), 0.0).astype(bf16)
    qk = (dot(qx, fold) * (HEAD_DIM**-0.5)).astype(bf16)
    wide_q = jnp.concatenate([qk] * 4, axis=1)
    own_seq = iota(wide_q.shape, 1) // 128 == (iota(wide_q.shape, 0) // heads) % 4
    wide_q = jnp.where(own_seq, wide_q.astype(f32), 0.0).astype(bf16)
    for g in range(rows // 4):
        for n in range(4 * g, 4 * g + 4):
            cache_c[n].wait()
        keys = jnp.concatenate([cache_v[n] for n in range(4 * g, 4 * g + 4)], axis=1)
        s_v[16 * g : 16 * g + 16, :] = dot(wide_q[16 * g : 16 * g + 16, :], keys, ((1,), (1,)))
    rid = iota((hr, 128), 0)
    lens = jnp.zeros((hr, 128), jnp.int32)
    bias = jnp.zeros((hr, 128), f32)
    len_c.wait()
    bias_c.wait()
    for n in range(rows):
        lens = jnp.where(rid // heads == n, len_ref[n], lens)
    for h in range(heads):
        bias = jnp.where(rid % heads == h, bias_ref[h], bias)
    later = ((iota((128, 256), 0) > iota((128, 256), 1)) | (iota((128, 256), 1) >= 128)).astype(bf16)
    blocks = span // 128
    usable, own, pieces = [], [], []
    for b in range(blocks):
        z = s_v[:, b * 128 : (b + 1) * 128] + bias
        ok = (iota((hr, 128), 1) + b * 128) < lens
        soft = jnp.log1p(jnp.exp(-jnp.abs(z)))
        usable.append(ok)
        own.append(jnp.minimum(z, 0.0) - soft)
        pieces.append(three_pieces(jnp.where(ok, -(jnp.maximum(z, 0.0) + soft), 0.0)))
    high, middle, low = [jnp.concatenate([p[i] for p in pieces], axis=0) for i in range(3)]
    both = (dot(low, later) + dot(middle, later)) + dot(high, later)
    beyond = jnp.zeros((hr, 128), f32)
    weights = [None] * blocks
    for b in range(blocks - 1, -1, -1):
        mine = both[b * hr : (b + 1) * hr, :]
        behind = mine[:, :128] + beyond
        beyond = beyond + mine[:, 128:]
        weights[b] = jnp.where(usable[b], jnp.exp(own[b] + behind), 0.0).astype(bf16)
    outs = []
    r16o = iota((16, 128), 0) // heads
    for g in range(rows // 4):
        pg = jnp.concatenate([w[16 * g : 16 * g + 16, :] for w in weights], axis=1)
        acc = None
        for i in range(4):
            o = dot(pg, cache_v[4 * g + i])
            acc = o if acc is None else jnp.where(r16o == i, o, acc)
        outs.append(acc)
    o = jnp.concatenate(outs, axis=0).astype(bf16)
    unfold = ((iota((128, 256), 0) - HEAD_DIM) == (iota((128, 256), 1) % HEAD_DIM)).astype(bf16)
    ox = jnp.where(lane // HEAD_DIM == row % heads, dot(o, unfold), 0.0).astype(bf16)
    collect = (iota((rows, hr), 1) // heads == iota((rows, hr), 0)).astype(bf16)
    heads_out = dot(collect, ox).astype(bf16)
    wo_c.wait()
    part_ref[...] = dot(heads_out, wo_v[...]).astype(bf16)
    for c in joins:
        c.wait()


def attend(tokens, lengths, cache, gain, wq, bias, wo, routes, shared_gate, shared_up):
    rows, d = tokens.shape
    n_pick = 8 * 64
    return call(
        attend_kernel, [((rows, d), bf16), ((n_pick, CAP * 8 * rows), bf16), ((1, shared_gate.shape[0], 256), bf16)],
        (lengths, bias, tokens, gain.reshape(1, -1), cache, wq, wo, routes, shared_gate, shared_up),
        in_specs=[HBM] * 10,
        scratch=[
            pltpu.SMEM(lengths.shape, jnp.int32), pltpu.SMEM(bias.shape, f32),
            pltpu.VMEM(tokens.shape, bf16), pltpu.VMEM((1, d), f32),
            pltpu.VMEM(cache.shape, bf16), pltpu.VMEM(wq.shape, bf16), pltpu.VMEM(wo.shape, bf16),
            pltpu.VMEM((4 * rows, cache.shape[1]), f32), pltpu.VMEM(routes.shape, jnp.int32),
            pltpu.SemaphoreType.DMA((rows,)), pltpu.SemaphoreType.DMA((9,)),
        ],
        limit_mib=16,
    )


def slots_of(routes_ref, rw_ref):
    top, rows = routes_ref.shape
    experts = 64
    hits = jnp.zeros((experts, rows), f32)
    weight = jnp.zeros((experts, rows), f32)
    which = iota((experts, rows), 0)
    for j in range(top):
        same = which == routes_ref[j : j + 1, :]
        hits = jnp.where(same, 1.0, hits)
        if rw_ref is not None:
            weight = jnp.where(same, rw_ref[j : j + 1, :], weight)
    before = (iota((rows, rows), 0) < iota((rows, rows), 1)).astype(bf16)
    rank = dot(hits.astype(bf16), before)
    slots = [jnp.where((hits > 0.5) & (rank == k), 1.0, 0.0) for k in range(CAP)]
    spread = (iota((8 * experts, experts), 0) // 8 == iota((8 * experts, experts), 1)).astype(bf16)
    return slots, weight, spread


def make_pick(routes_ref, pick_ref):
    rows = routes_ref.shape[1]
    slots, _, spread = slots_of(routes_ref, None)
    n = spread.shape[0]
    tile = (iota((rows, 8 * rows), 0) == iota((rows, 8 * rows), 1) % rows).astype(bf16)
    here = (iota((n, 8 * rows), 0) % 8) == (iota((n, 8 * rows), 1) // rows)
    for k in range(CAP):
        wide = dot(slots[k].astype(bf16), tile).astype(bf16)
        full = jnp.where(here, dot(spread, wide), 0.0)
        pick_ref[:, k * 8 * rows : (k + 1) * 8 * rows] = full.astype(bf16)


def mix_kernel(part_ref, tok_ref, p0, p1, p2, p3, gain_ref, pick_ref, normed_hbm, residual_hbm, sent_hbm,
               normed_v, residual_v, sent_v, sems):
    rows, d = tok_ref.shape
    wide = d // 8
    quarter = residual_hbm.shape[1]
    total = (p0[...].astype(f32) + p1[...].astype(f32)) + (p2[...].astype(f32) + p3[...].astype(f32))
    residual = tok_ref[...].astype(f32) + total
    residual_v[...] = residual
    ms = jnp.mean(residual * residual, axis=-1, keepdims=True)
    normed = (residual * lax.rsqrt(ms + EPS) * gain_ref[...]).astype(bf16)
    normed_v[...] = normed
    mine = pl.ds(pl.multiple_of(part_ref[0] * quarter, quarter), quarter)
    copies = copy_all([(normed_v, normed_hbm), (residual_v.at[:, mine], residual_hbm)], sems)
    stacked = jnp.concatenate([normed[:, r * wide : (r + 1) * wide] for r in range(8)], axis=0)
    for k in range(CAP):
        pick = pick_ref[:, k * 8 * rows : (k + 1) * 8 * rows]
        cols = slice(k * wide, (k + 1) * wide)
        sent_v[:, cols] = dot(pick, stacked).astype(bf16)
        copies += copy_all([(sent_v.at[:, cols], sent_hbm.at[:, cols])], sems, 2 + k)
    for c in copies:
        c.wait()


def stack_kernel(near_ref, low_ref, high_ref, out_ref):
    out_ref[0:3] = near_ref[...]
    out_ref[3:6] = low_ref[...]
    out_ref[6:8] = high_ref[0:2]


def cut_kernel(part_ref, down_hbm, shared_hbm, o0, o1, o2, o3, all_v, sems):
    outs = (o0, o1, o2, o3)
    quarter = o0.shape[1]
    f = down_hbm.shape[1]
    first = copy_all([(down_hbm.at[0], all_v.at[:f, :]), (shared_hbm, all_v.at[f:, :])], sems, 4)
    for c in first:
        c.wait()
    pairs = []
    for k in (1, 3, 2, 0):
        cols = pl.ds(pl.multiple_of(((part_ref[0] + k) % 4) * quarter, quarter), quarter)
        pairs.append((all_v.at[:, cols], outs[k]))
    for c in copy_all(pairs, sems):
        c.wait()


def silu(v):
    return v / (1.0 + jnp.exp(-v))


def shared_kernel(ep_ref, normed_ref, b0, b1, b2, b3, b4, b5, b6, b7, hidden_ref):
    blocks = (b0, b1, b2, b3, b4, b5, b6, b7)
    rows, d = normed_ref.shape
    wide = d // 8
    ep = ep_ref[0]
    z = ep // 8
    y = (ep // 2) % 4
    c = ep % 2
    lane = iota((wide, wide), 1)
    there = ((y + 4 - lane // 64) % 4) * 64 + ((c + lane // 32) % 2) * 32 + lane % 32
    order = (iota((wide, wide), 0) == there).astype(bf16)
    cols = [normed_ref[:, pl.ds(pl.multiple_of(((z + 8 + j) % 8) * wide, wide), wide)] for j in Z_ORDER]
    mine = dot(jnp.concatenate(cols, axis=0), order).astype(bf16)
    n = b0.shape[2]
    acc = jnp.zeros((rows, n), f32)
    for j in range(8):
        w = jnp.concatenate([b[j] for b in blocks], axis=0)
        acc = acc + dot(mine[j * rows : (j + 1) * rows, :], w)
    half = n // 2
    hidden = silu(acc[:, :half]) * acc[:, half:]
    hidden_ref[...] = hidden.astype(bf16)


def expert_kernel(arrived_ref, wg_ref, wu_ref, hidden_ref, x_v):
    n = arrived_ref.shape[0]
    peers = n // 8
    wide = arrived_ref.shape[1] // CAP
    a = iota((n, n), 0)
    b = iota((n, n), 1)
    order = ((b // 8 == a % peers) & (b % 8 == a // peers)).astype(bf16)
    sorted_rows = dot(order, arrived_ref[...]).astype(bf16)
    for r in range(8):
        for k in range(CAP):
            x_v[k * peers : (k + 1) * peers, r * wide : (r + 1) * wide] = sorted_rows[
                r * peers : (r + 1) * peers, k * wide : (k + 1) * wide
            ]
    x = x_v[...]
    gate = dot(x, wg_ref[0])
    up = dot(x, wu_ref[0])
    hidden_ref[...] = (silu(gate) * up).astype(bf16)


def down_kernel(h0, h1, h2, h3, w0, w1, w2, w3, back_ref, w_v, sems):
    n = back_ref.shape[0]
    peers = n // 8
    f = h0.shape[1]
    m = CAP * peers
    copies = copy_all([(w.at[:f, :], w_v.at[k]) for k, w in enumerate((w0, w1, w2, w3))], sems)
    a = iota((n, 2 * m), 0)
    b = iota((n, 2 * m), 1)
    order = ((a % 8 == b // peers) & (a // 8 == b % peers)).astype(bf16)
    acc = None
    for k, h in enumerate((h0, h1, h2, h3)):
        copies[k].wait()
        part = dot(h[:m, :], w_v[k])
        acc = part if acc is None else acc + part
    out = acc.astype(bf16)
    half = out.shape[1] // 2
    pieces = [
        out[k * peers : (k + 1) * peers, h * half : (h + 1) * half] for k in range(CAP) for h in range(2)
    ]
    rhs = jnp.concatenate(pieces, axis=0)
    back_ref[...] = dot(order, rhs).astype(bf16)


def side_kernel(routes_ref, rw_ref, tok_hbm, gain_ref, kw_hbm, vw_hbm, mixed_hbm, gv_ref,
                mix_ref, kv_ref, gate_ref, tok_ref, both_ref, mixed_ref, sems):
    rows = tok_ref.shape[0]
    n = kw_hbm.shape[0]
    copies = copy_all([(tok_hbm, tok_ref), (kw_hbm, both_ref.at[:n, :]), (vw_hbm, both_ref.at[n:, :]),
                       (mixed_hbm, mixed_ref)], sems)
    for c in copies:
        c.wait()
    x = tok_ref[...].astype(f32)
    ms = jnp.mean(x * x, axis=-1, keepdims=True)
    normed = (x * lax.rsqrt(ms + EPS) * gain_ref[...]).astype(bf16)
    kv_ref[...] = dot(normed, both_ref[...], ((1,), (1,))).astype(bf16)
    slots, weight, spread = slots_of(routes_ref, rw_ref)
    lane = iota((rows, spread.shape[0]), 1) % 8
    mixed = [jnp.zeros(lane.shape, f32) for _ in range(3)]
    for k in range(CAP):
        for i, piece in enumerate(three_pieces(slots[k] * weight)):
            mixed[i] = jnp.where(lane // 2 == k, dot(piece, spread, ((0,), (1,))), mixed[i])
    for h in range(2):
        for i in range(3):
            row = (h * 3 + i) * rows
            mix_ref[row : row + rows, :] = jnp.where(lane % 2 == h, mixed[i], 0.0).astype(bf16)
    total = jnp.zeros((rows, 128), f32)
    for j in range(gv_ref.shape[0]):
        total = total + mixed_ref[:, j * 128 : (j + 1) * 128].astype(f32) * gv_ref[j : j + 1, :].astype(f32)
    logit = jnp.sum(total, axis=-1, keepdims=True)
    gate_ref[...] = jnp.broadcast_to(1.0 / (1.0 + jnp.exp(-logit)), gate_ref.shape)


def base_kernel(residual_hbm, gate_ref, s0, s1, s2, s3, w0, w1, w2, w3, base_ref, residual_v, w_v, sems):
    at = w0.shape[0] - w_v.shape[1]
    copies = copy_all([(w.at[at:, :], w_v.at[k]) for k, w in enumerate((w0, w1, w2, w3))], sems)
    copies += copy_all([(residual_hbm, residual_v)], sems, 4)
    acc = None
    for k, h in enumerate((s0, s1, s2, s3)):
        copies[k].wait()
        part = dot(h[h.shape[0] - base_ref.shape[0] :, : w_v.shape[1]], w_v[k])
        acc = part if acc is None else acc + part
    copies[4].wait()
    base_ref[...] = residual_v[...] + gate_ref[:, :1] * acc


def final_kernel(back_ref, mix_ref, base_ref, out_ref):
    rows = out_ref.shape[0]
    half = out_ref.shape[1] // 2
    for h in range(2):
        r = dot(mix_ref[h * 3 * rows : (h + 1) * 3 * rows, :], back_ref[...])
        routed = (r[2 * rows :] + r[rows : 2 * rows]) + r[:rows]
        cols = slice(h * half, (h + 1) * half)
        out_ref[:, cols] = (base_ref[:, cols] + routed).astype(bf16)


def around(k, size):
    return [(i, (i + k) % size) for i in range(size)]


def after(value, *deps):
    return lax.optimization_barrier((value, *deps))[0]


def shards(
    tokens, lengths, cache, attn_gain, query_weight, key_weight, value_weight, stick_bias, out_weight,
    ffn_gain, routes, route_weights, expert_gate, expert_up, expert_down, shared_gate, shared_up,
    shared_down, gate_vector,
):
    ntp = lax.axis_size("tp")
    nep = lax.axis_size("ep")
    rows, d = tokens.shape
    quarter = d // ntp
    part = lax.axis_index("tp").reshape(1)
    n_pick = 8 * nep

    def shift(value, dz, dy, dc):
        perm = []
        for i in range(nep):
            z, y, c = i // 8, i // 2 % 4, i % 2
            perm.append((i, (z + dz) % (nep // 8) * 8 + (y + dy) % 4 * 2 + (c + dc) % 2))
        return lax.ppermute(value, "ep", perm)

    partial, pick, joined = attend(
        tokens, lengths, cache, attn_gain, query_weight, stick_bias, out_weight, routes.T, shared_gate, shared_up
    )
    others = [lax.ppermute(partial, "tp", around(k, ntp)) for k in (2, 1, 3)]
    near = [joined, shift(joined, 1, 0, 0), shift(joined, -1, 0, 0)]
    normed_mix, residual, sent = call(
        mix_kernel, [((rows, d), bf16), ((rows, quarter), f32), ((n_pick, CAP * d // 8), bf16)],
        (part, tokens, partial, *others, ffn_gain.reshape(1, -1), pick),
        in_specs=[SM] + [VM] * 7, out_specs=[HBM] * 3,
        scratch=[pltpu.VMEM((rows, d), bf16), pltpu.VMEM((rows, d), f32),
                 pltpu.VMEM((n_pick, CAP * d // 8), bf16), pltpu.SemaphoreType.DMA((5,))],
    )
    arrived = lax.all_to_all(sent.reshape(nep, 8, -1), "ep", 0, 0, tiled=True)
    arrived = arrived.reshape(n_pick, -1)
    near = jnp.concatenate(after(near, sent))
    low, high = shift(near, 3, 0, 0), shift(near, -3, 0, 0)
    f = expert_down.shape[1] + shared_down.shape[0]
    cuts = call(
        cut_kernel, [((f, quarter), bf16)] * 4, (part, after(expert_down, sent), shared_down),
        in_specs=[SM, HBM, HBM], out_specs=[HBM] * 4,
        scratch=[pltpu.VMEM((f, d), bf16), pltpu.SemaphoreType.DMA((6,))],
    )
    downs = [cuts[0]] + [lax.ppermute(cuts[k], "tp", around(k, ntp)) for k in range(1, ntp)]
    mix, new_kv, mix_gate = call(
        side_kernel,
        [((6 * rows, n_pick), bf16), ((rows, 2 * HEAD_DIM), bf16), ((rows, 128), f32)],
        (routes.T, route_weights.T, after(tokens, sent), attn_gain.reshape(1, -1), key_weight.T, value_weight.T,
         normed_mix, gate_vector.reshape(-1, 128)),
        in_specs=[VM, VM, HBM, VM, HBM, HBM, HBM, VM],
        scratch=[pltpu.VMEM((rows, d), bf16), pltpu.VMEM((2 * HEAD_DIM, d), bf16), pltpu.VMEM((rows, d), bf16),
                 pltpu.SemaphoreType.DMA((4,))],
    )
    m = CAP * nep
    (hidden,) = call(
        expert_kernel, [((m, expert_gate.shape[2]), bf16)],
        (arrived, expert_gate, expert_up), scratch=[pltpu.VMEM((m, d), bf16)],
    )
    hiddens = [hidden] + [lax.ppermute(hidden, "tp", around(k, ntp)) for k in range(1, ntp)]
    (column,) = call(stack_kernel, [((8, *joined.shape[1:]), bf16)], (after(near, hidden), low, high))
    planes = [column] + [shift(column, 0, k, 0) for k in range(1, 4)]
    blocks = [column, shift(column, 0, 0, 1)]
    (back,) = call(
        down_kernel, [((n_pick, quarter // 2), bf16)], (*hiddens, *downs), in_specs=[VM] * 4 + [HBM] * 4,
        scratch=[pltpu.VMEM((ntp, expert_down.shape[1], quarter), bf16), pltpu.SemaphoreType.DMA((4,))],
    )
    returned = lax.all_to_all(back.reshape(nep, 8, -1), "ep", 0, 0, tiled=True)
    returned = returned.reshape(n_pick, -1)
    for block in planes[1:]:
        blocks += [block, shift(block, 0, 0, 1)]
    (shared_hidden,) = call(
        shared_kernel, [((rows, shared_gate.shape[1]), bf16)],
        (lax.axis_index("ep").reshape(1), after(normed_mix, back), *blocks), in_specs=[SM] + [VM] * 9,
    )
    smalls = [shared_hidden] + [lax.ppermute(shared_hidden, "tp", around(k, ntp)) for k in range(1, ntp)]
    (base,) = call(
        base_kernel, [((rows, quarter), f32)], (after(residual, back), mix_gate, *smalls, *downs),
        in_specs=[HBM] + [VM] * 5 + [HBM] * 4,
        scratch=[pltpu.VMEM((rows, quarter), f32), pltpu.VMEM((ntp, shared_down.shape[0], quarter), bf16),
                 pltpu.SemaphoreType.DMA((5,))],
    )
    (layer_out,) = call(final_kernel, [((rows, quarter), bf16)], (returned, mix, base))
    return (layer_out, new_kv)


def solution(mesh):
    placed = (
        P("ep", None), P("ep"), P("ep", None, "tp"), P(), P(None, "tp"), P(None, "tp"), P(None, "tp"),
        P("tp"), P("tp", None), P(), P("ep", None), P("ep", None), P("ep", None, "tp"),
        P("ep", None, "tp"), P("ep", "tp", None), P("ep", "tp"), P("ep", "tp"), P("tp", None), P(),
    )

    return jax.shard_map(shards, mesh=mesh, in_specs=placed, out_specs=(P("ep", "tp"), P("ep", "tp")), check_vma=False)
```

```python
import jax
import jax.numpy as jnp
from jax import lax
from jax.experimental import pallas as pl
from jax.experimental.pallas import tpu as pltpu
from jax.sharding import PartitionSpec as P

HEAD_DIM = 64
EPS = 1e-06
CAP = 3
Z_ORDER = (0, -1, 1, -3, -4, -2, 3, 2)
bf16 = jnp.bfloat16
f32 = jnp.float32

VM = pl.BlockSpec(memory_space=pltpu.VMEM)
SM = pl.BlockSpec(memory_space=pltpu.SMEM)
HBM = pl.BlockSpec(memory_space=pltpu.HBM)


def iota(shape, dim):
    return lax.broadcasted_iota(jnp.int32, shape, dim)


def dot(a, b, dims=((1,), (0,))):
    return lax.dot_general(a, b, (dims, ((), ())), preferred_element_type=f32)


def three_pieces(values):
    high = values.astype(bf16)
    rest = values - high.astype(f32)
    middle = rest.astype(bf16)
    low = (rest - middle.astype(f32)).astype(bf16)
    return high, middle, low


def hbm(value):
    return pltpu.with_memory_space_constraint(value, pltpu.HBM)


def call(kernel, outs, ins, in_specs=None, out_specs=None, scratch=(), limit_mib=8):
    in_specs = in_specs or [VM] * len(ins)
    out_specs = out_specs or [VM] * len(outs)
    ins = [hbm(x) if spec is HBM else x for x, spec in zip(ins, in_specs)]
    shapes = [
        pltpu.HBM(s, t) if spec is HBM else jax.ShapeDtypeStruct(s, t) for (s, t), spec in zip(outs, out_specs)
    ]
    return pl.pallas_call(
        kernel,
        out_shape=tuple(shapes),
        in_specs=in_specs,
        out_specs=tuple(out_specs),
        scratch_shapes=list(scratch),
        compiler_params=pltpu.CompilerParams(vmem_limit_bytes=limit_mib * 1024 * 1024),
    )(*ins)


def copy_all(pairs, sems, first=0):
    copies = [pltpu.make_async_copy(src, dst, sems.at[first + i]) for i, (src, dst) in enumerate(pairs)]
    for c in copies:
        c.start()
    return copies


def attend_kernel(len_hbm, bias_hbm, tok_hbm, gain_hbm, cache_hbm, wq_hbm, wo_hbm, routes_hbm, sg_hbm, su_hbm,
                  part_ref, pick_ref, joined_ref,
                  len_ref, bias_ref, tok_ref, gain_ref, cache_v, wq_v, wo_v, s_v, routes_v, sem_c, sem_w):
    rows = tok_ref.shape[0]
    span = cache_v.shape[1]
    heads = 4
    hr = rows * heads
    small = []
    for i, (src, dst) in enumerate(
        [(tok_hbm, tok_ref), (gain_hbm, gain_ref), (wq_hbm, wq_v), (wo_hbm, wo_v),
         (len_hbm, len_ref), (bias_hbm, bias_ref)]
    ):
        small.append(pltpu.make_async_copy(src, dst, sem_w.at[i]))
    tok_c, gain_c, wq_c, wo_c, len_c, bias_c = small
    routes_c = pltpu.make_async_copy(routes_hbm, routes_v, sem_w.at[6])
    routes_c.start()
    tok_c.start()
    gain_c.start()
    wq_c.start()
    cache_c = []
    for n in range(rows):
        c = pltpu.make_async_copy(cache_hbm.at[n], cache_v.at[n], sem_c.at[n])
        c.start()
        cache_c.append(c)
    len_c.start()
    bias_c.start()
    wo_c.start()
    half = sg_hbm.shape[1]
    joins = copy_all([(sg_hbm, joined_ref.at[0, :, :half]), (su_hbm, joined_ref.at[0, :, half:])], sem_w, 7)
    routes_c.wait()
    make_pick(routes_v, pick_ref)
    tok_c.wait()
    gain_c.wait()
    x = tok_ref[...].astype(f32)
    ms = jnp.mean(x * x, axis=-1, keepdims=True)
    normed = (x * lax.rsqrt(ms + EPS) * gain_ref[...]).astype(bf16)
    expand = (iota((hr, rows), 0) // heads == iota((hr, rows), 1)).astype(bf16)
    lane = iota((hr, heads * HEAD_DIM), 1)
    row = iota((hr, heads * HEAD_DIM), 0)
    fold = ((iota((256, 128), 0) % HEAD_DIM) == iota((256, 128), 1)).astype(bf16)
    wq_c.wait()
    q = dot(normed, wq_v[...]).astype(bf16)
    qx = jnp.where(lane // HEAD_DIM == row % heads, dot(expand, q), 0.0).astype(bf16)
    qk = (dot(qx, fold) * (HEAD_DIM**-0.5)).astype(bf16)
    wide_q = jnp.concatenate([qk] * 4, axis=1)
    own_seq = iota(wide_q.shape, 1) // 128 == (iota(wide_q.shape, 0) // heads) % 4
    wide_q = jnp.where(own_seq, wide_q.astype(f32), 0.0).astype(bf16)
    for g in range(rows // 4):
        for n in range(4 * g, 4 * g + 4):
            cache_c[n].wait()
        keys = jnp.concatenate([cache_v[n] for n in range(4 * g, 4 * g + 4)], axis=1)
        s_v[16 * g : 16 * g + 16, :] = dot(wide_q[16 * g : 16 * g + 16, :], keys, ((1,), (1,)))
    rid = iota((hr, 128), 0)
    lens = jnp.zeros((hr, 128), jnp.int32)
    bias = jnp.zeros((hr, 128), f32)
    len_c.wait()
    bias_c.wait()
    for n in range(rows):
        lens = jnp.where(rid // heads == n, len_ref[n], lens)
    for h in range(heads):
        bias = jnp.where(rid % heads == h, bias_ref[h], bias)
    later = ((iota((128, 256), 0) > iota((128, 256), 1)) | (iota((128, 256), 1) >= 128)).astype(bf16)
    blocks = span // 128
    usable, own, pieces = [], [], []
    for b in range(blocks):
        z = s_v[:, b * 128 : (b + 1) * 128] + bias
        ok = (iota((hr, 128), 1) + b * 128) < lens
        soft = jnp.log1p(jnp.exp(-jnp.abs(z)))
        usable.append(ok)
        own.append(jnp.minimum(z, 0.0) - soft)
        pieces.append(three_pieces(jnp.where(ok, -(jnp.maximum(z, 0.0) + soft), 0.0)))
    high, middle, low = [jnp.concatenate([p[i] for p in pieces], axis=0) for i in range(3)]
    both = (dot(low, later) + dot(middle, later)) + dot(high, later)
    beyond = jnp.zeros((hr, 128), f32)
    weights = [None] * blocks
    for b in range(blocks - 1, -1, -1):
        mine = both[b * hr : (b + 1) * hr, :]
        behind = mine[:, :128] + beyond
        beyond = beyond + mine[:, 128:]
        weights[b] = jnp.where(usable[b], jnp.exp(own[b] + behind), 0.0).astype(bf16)
    outs = []
    r16o = iota((16, 128), 0) // heads
    for g in range(rows // 4):
        pg = jnp.concatenate([w[16 * g : 16 * g + 16, :] for w in weights], axis=1)
        acc = None
        for i in range(4):
            o = dot(pg, cache_v[4 * g + i])
            acc = o if acc is None else jnp.where(r16o == i, o, acc)
        outs.append(acc)
    o = jnp.concatenate(outs, axis=0).astype(bf16)
    unfold = ((iota((128, 256), 0) - HEAD_DIM) == (iota((128, 256), 1) % HEAD_DIM)).astype(bf16)
    ox = jnp.where(lane // HEAD_DIM == row % heads, dot(o, unfold), 0.0).astype(bf16)
    collect = (iota((rows, hr), 1) // heads == iota((rows, hr), 0)).astype(bf16)
    heads_out = dot(collect, ox).astype(bf16)
    wo_c.wait()
    part_ref[...] = dot(heads_out, wo_v[...]).astype(bf16)
    for c in joins:
        c.wait()


def attend(tokens, lengths, cache, gain, wq, bias, wo, routes, shared_gate, shared_up):
    rows, d = tokens.shape
    n_pick = 8 * 64
    return call(
        attend_kernel, [((rows, d), bf16), ((n_pick, CAP * 8 * rows), bf16), ((1, shared_gate.shape[0], 256), bf16)],
        (lengths, bias, tokens, gain.reshape(1, -1), cache, wq, wo, routes, shared_gate, shared_up),
        in_specs=[HBM] * 10,
        scratch=[
            pltpu.SMEM(lengths.shape, jnp.int32), pltpu.SMEM(bias.shape, f32),
            pltpu.VMEM(tokens.shape, bf16), pltpu.VMEM((1, d), f32),
            pltpu.VMEM(cache.shape, bf16), pltpu.VMEM(wq.shape, bf16), pltpu.VMEM(wo.shape, bf16),
            pltpu.VMEM((4 * rows, cache.shape[1]), f32), pltpu.VMEM(routes.shape, jnp.int32),
            pltpu.SemaphoreType.DMA((rows,)), pltpu.SemaphoreType.DMA((9,)),
        ],
        limit_mib=16,
    )


def slots_of(routes_ref, rw_ref):
    top, rows = routes_ref.shape
    experts = 64
    hits = jnp.zeros((experts, rows), f32)
    weight = jnp.zeros((experts, rows), f32)
    which = iota((experts, rows), 0)
    for j in range(top):
        same = which == routes_ref[j : j + 1, :]
        hits = jnp.where(same, 1.0, hits)
        if rw_ref is not None:
            weight = jnp.where(same, rw_ref[j : j + 1, :], weight)
    before = (iota((rows, rows), 0) < iota((rows, rows), 1)).astype(bf16)
    rank = dot(hits.astype(bf16), before)
    slots = [jnp.where((hits > 0.5) & (rank == k), 1.0, 0.0) for k in range(CAP)]
    spread = (iota((8 * experts, experts), 0) // 8 == iota((8 * experts, experts), 1)).astype(bf16)
    return slots, weight, spread


def make_pick(routes_ref, pick_ref):
    rows = routes_ref.shape[1]
    slots, _, spread = slots_of(routes_ref, None)
    n = spread.shape[0]
    tile = (iota((rows, 8 * rows), 0) == iota((rows, 8 * rows), 1) % rows).astype(bf16)
    here = (iota((n, 8 * rows), 0) % 8) == (iota((n, 8 * rows), 1) // rows)
    for k in range(CAP):
        wide = dot(slots[k].astype(bf16), tile).astype(bf16)
        full = jnp.where(here, dot(spread, wide), 0.0)
        pick_ref[:, k * 8 * rows : (k + 1) * 8 * rows] = full.astype(bf16)


def mix_kernel(part_ref, tok_ref, p0, p1, p2, p3, gain_ref, pick_ref, normed_hbm, residual_hbm, sent_hbm,
               normed_v, residual_v, sent_v, sems):
    rows, d = tok_ref.shape
    wide = d // 8
    quarter = residual_hbm.shape[1]
    total = (p0[...].astype(f32) + p1[...].astype(f32)) + (p2[...].astype(f32) + p3[...].astype(f32))
    residual = tok_ref[...].astype(f32) + total
    residual_v[...] = residual
    ms = jnp.mean(residual * residual, axis=-1, keepdims=True)
    normed = (residual * lax.rsqrt(ms + EPS) * gain_ref[...]).astype(bf16)
    normed_v[...] = normed
    mine = pl.ds(pl.multiple_of(part_ref[0] * quarter, quarter), quarter)
    copies = copy_all([(normed_v, normed_hbm), (residual_v.at[:, mine], residual_hbm)], sems)
    stacked = jnp.concatenate([normed[:, r * wide : (r + 1) * wide] for r in range(8)], axis=0)
    for k in range(CAP):
        pick = pick_ref[:, k * 8 * rows : (k + 1) * 8 * rows]
        cols = slice(k * wide, (k + 1) * wide)
        sent_v[:, cols] = dot(pick, stacked).astype(bf16)
        copies += copy_all([(sent_v.at[:, cols], sent_hbm.at[:, cols])], sems, 2 + k)
    for c in copies:
        c.wait()


def stack_kernel(near_ref, low_ref, high_ref, out_ref):
    out_ref[0:3] = near_ref[...]
    out_ref[3:6] = low_ref[...]
    out_ref[6:8] = high_ref[0:2]


def cut_kernel(part_ref, down_hbm, o0, o1, o2, o3, all_v, sems):
    outs = (o0, o1, o2, o3)
    quarter = o0.shape[1]
    for c in copy_all([(down_hbm.at[0], all_v)], sems, 4):
        c.wait()
    pairs = []
    for k in (1, 3, 2, 0):
        cols = pl.ds(pl.multiple_of(((part_ref[0] + k) % 4) * quarter, quarter), quarter)
        pairs.append((all_v.at[:, cols], outs[k]))
    for c in copy_all(pairs, sems):
        c.wait()


def silu(v):
    return v / (1.0 + jnp.exp(-v))


def shared_kernel(at_ref, normed_ref, down_ref, residual_hbm, gate_ref, b0, b1, b2, b3, b4, b5, b6, b7,
                  base_ref, o1, o2, o3, all_v, residual_v, sem):
    blocks = (b0, b1, b2, b3, b4, b5, b6, b7)
    rows, d = normed_ref.shape
    wide = d // 8
    fetch = pltpu.make_async_copy(residual_hbm, residual_v, sem)
    fetch.start()
    ep = at_ref[0]
    z = ep // 8
    y = (ep // 2) % 4
    c = ep % 2
    lane = iota((wide, wide), 1)
    there = ((y + 4 - lane // 64) % 4) * 64 + ((c + lane // 32) % 2) * 32 + lane % 32
    order = (iota((wide, wide), 0) == there).astype(bf16)
    cols = [normed_ref[:, pl.ds(pl.multiple_of(((z + 8 + j) % 8) * wide, wide), wide)] for j in Z_ORDER]
    mine = dot(jnp.concatenate(cols, axis=0), order).astype(bf16)
    n = b0.shape[2]
    acc = jnp.zeros((rows, n), f32)
    for j in range(8):
        w = jnp.concatenate([b[j] for b in blocks], axis=0)
        acc = acc + dot(mine[j * rows : (j + 1) * rows, :], w)
    half = n // 2
    hidden = silu(acc[:, :half]) * acc[:, half:]
    all_v[...] = dot(hidden.astype(bf16), down_ref[...])
    quarter = o1.shape[1]
    cols = [pl.ds(pl.multiple_of(((at_ref[1] + k) % 4) * quarter, quarter), quarter) for k in range(4)]
    for k, o in enumerate((o1, o2, o3)):
        o[...] = all_v[:, cols[k + 1]].astype(bf16)
    fetch.wait()
    base_ref[...] = residual_v[...] + gate_ref[:, :1] * all_v[:, cols[0]]


def expert_kernel(arrived_ref, wg_ref, wu_ref, hidden_ref, x_v):
    n = arrived_ref.shape[0]
    peers = n // 8
    wide = arrived_ref.shape[1] // CAP
    a = iota((n, n), 0)
    b = iota((n, n), 1)
    order = ((b // 8 == a % peers) & (b % 8 == a // peers)).astype(bf16)
    sorted_rows = dot(order, arrived_ref[...]).astype(bf16)
    for r in range(8):
        for k in range(CAP):
            x_v[k * peers : (k + 1) * peers, r * wide : (r + 1) * wide] = sorted_rows[
                r * peers : (r + 1) * peers, k * wide : (k + 1) * wide
            ]
    x = x_v[...]
    gate = dot(x, wg_ref[0])
    up = dot(x, wu_ref[0])
    hidden_ref[...] = (silu(gate) * up).astype(bf16)


def down_kernel(h0, h1, h2, h3, w0, w1, w2, w3, back_ref, w_v, sems):
    n = back_ref.shape[0]
    peers = n // 8
    m = CAP * peers
    copies = copy_all([(w, w_v.at[k]) for k, w in enumerate((w0, w1, w2, w3))], sems)
    a = iota((n, 2 * m), 0)
    b = iota((n, 2 * m), 1)
    order = ((a % 8 == b // peers) & (a // 8 == b % peers)).astype(bf16)
    acc = None
    for k, h in enumerate((h0, h1, h2, h3)):
        copies[k].wait()
        part = dot(h[:m, :], w_v[k])
        acc = part if acc is None else acc + part
    out = acc.astype(bf16)
    half = out.shape[1] // 2
    pieces = [
        out[k * peers : (k + 1) * peers, h * half : (h + 1) * half] for k in range(CAP) for h in range(2)
    ]
    rhs = jnp.concatenate(pieces, axis=0)
    back_ref[...] = dot(order, rhs).astype(bf16)


def side_kernel(routes_ref, rw_ref, tok_hbm, gain_ref, kw_hbm, vw_hbm, mixed_hbm, gv_ref,
                mix_ref, kv_ref, gate_ref, tok_ref, both_ref, mixed_ref, sems):
    rows = tok_ref.shape[0]
    n = kw_hbm.shape[0]
    copies = copy_all([(tok_hbm, tok_ref), (kw_hbm, both_ref.at[:n, :]), (vw_hbm, both_ref.at[n:, :]),
                       (mixed_hbm, mixed_ref)], sems)
    for c in copies:
        c.wait()
    x = tok_ref[...].astype(f32)
    ms = jnp.mean(x * x, axis=-1, keepdims=True)
    normed = (x * lax.rsqrt(ms + EPS) * gain_ref[...]).astype(bf16)
    kv_ref[...] = dot(normed, both_ref[...], ((1,), (1,))).astype(bf16)
    slots, weight, spread = slots_of(routes_ref, rw_ref)
    lane = iota((rows, spread.shape[0]), 1) % 8
    mixed = [jnp.zeros(lane.shape, f32) for _ in range(3)]
    for k in range(CAP):
        for i, piece in enumerate(three_pieces(slots[k] * weight)):
            mixed[i] = jnp.where(lane // 2 == k, dot(piece, spread, ((0,), (1,))), mixed[i])
    for h in range(2):
        for i in range(3):
            row = (h * 3 + i) * rows
            mix_ref[row : row + rows, :] = jnp.where(lane % 2 == h, mixed[i], 0.0).astype(bf16)
    total = jnp.zeros((rows, 128), f32)
    for j in range(gv_ref.shape[0]):
        total = total + mixed_ref[:, j * 128 : (j + 1) * 128].astype(f32) * gv_ref[j : j + 1, :].astype(f32)
    logit = jnp.sum(total, axis=-1, keepdims=True)
    gate_ref[...] = jnp.broadcast_to(1.0 / (1.0 + jnp.exp(-logit)), gate_ref.shape)


def final_kernel(back_ref, mix_ref, gate_ref, base_ref, s1, s2, s3, out_ref):
    rows = out_ref.shape[0]
    half = out_ref.shape[1] // 2
    shared = s1[...].astype(f32) + (s2[...].astype(f32) + s3[...].astype(f32))
    base = base_ref[...] + gate_ref[:, :1] * shared
    for h in range(2):
        r = dot(mix_ref[h * 3 * rows : (h + 1) * 3 * rows, :], back_ref[...])
        routed = (r[2 * rows :] + r[rows : 2 * rows]) + r[:rows]
        cols = slice(h * half, (h + 1) * half)
        out_ref[:, cols] = (base[:, cols] + routed).astype(bf16)


def around(k, size):
    return [(i, (i + k) % size) for i in range(size)]


def after(value, *deps):
    return lax.optimization_barrier((value, *deps))[0]


def shards(
    tokens, lengths, cache, attn_gain, query_weight, key_weight, value_weight, stick_bias, out_weight,
    ffn_gain, routes, route_weights, expert_gate, expert_up, expert_down, shared_gate, shared_up,
    shared_down, gate_vector,
):
    ntp = lax.axis_size("tp")
    nep = lax.axis_size("ep")
    rows, d = tokens.shape
    quarter = d // ntp
    part = lax.axis_index("tp").reshape(1)
    n_pick = 8 * nep

    def shift(value, dz, dy, dc):
        perm = []
        for i in range(nep):
            z, y, c = i // 8, i // 2 % 4, i % 2
            perm.append((i, (z + dz) % (nep // 8) * 8 + (y + dy) % 4 * 2 + (c + dc) % 2))
        return lax.ppermute(value, "ep", perm)

    partial, pick, joined = attend(
        tokens, lengths, cache, attn_gain, query_weight, stick_bias, out_weight, routes.T, shared_gate, shared_up
    )
    others = [lax.ppermute(partial, "tp", around(k, ntp)) for k in (2, 1, 3)]
    near = [joined, shift(joined, 1, 0, 0), shift(joined, -1, 0, 0)]
    normed_mix, residual, sent = call(
        mix_kernel, [((rows, d), bf16), ((rows, quarter), f32), ((n_pick, CAP * d // 8), bf16)],
        (part, tokens, partial, *others, ffn_gain.reshape(1, -1), pick),
        in_specs=[SM] + [VM] * 7, out_specs=[HBM] * 3,
        scratch=[pltpu.VMEM((rows, d), bf16), pltpu.VMEM((rows, d), f32),
                 pltpu.VMEM((n_pick, CAP * d // 8), bf16), pltpu.SemaphoreType.DMA((5,))],
    )
    arrived = lax.all_to_all(sent.reshape(nep, 8, -1), "ep", 0, 0, tiled=True)
    arrived = arrived.reshape(n_pick, -1)
    near = jnp.concatenate(after(near, sent))
    low, high = shift(near, 3, 0, 0), shift(near, -3, 0, 0)
    f = expert_down.shape[1]
    cuts = call(
        cut_kernel, [((f, quarter), bf16)] * 4, (part, after(expert_down, sent)),
        in_specs=[SM, HBM], out_specs=[HBM] * 4,
        scratch=[pltpu.VMEM((f, d), bf16), pltpu.SemaphoreType.DMA((5,))],
    )
    downs = [cuts[0]] + [lax.ppermute(cuts[k], "tp", around(k, ntp)) for k in range(1, ntp)]
    mix, new_kv, mix_gate = call(
        side_kernel,
        [((6 * rows, n_pick), bf16), ((rows, 2 * HEAD_DIM), bf16), ((rows, 128), f32)],
        (routes.T, route_weights.T, after(tokens, sent), attn_gain.reshape(1, -1), key_weight.T, value_weight.T,
         normed_mix, gate_vector.reshape(-1, 128)),
        in_specs=[VM, VM, HBM, VM, HBM, HBM, HBM, VM],
        scratch=[pltpu.VMEM((rows, d), bf16), pltpu.VMEM((2 * HEAD_DIM, d), bf16), pltpu.VMEM((rows, d), bf16),
                 pltpu.SemaphoreType.DMA((4,))],
    )
    m = CAP * nep
    (hidden,) = call(
        expert_kernel, [((m, expert_gate.shape[2]), bf16)],
        (arrived, expert_gate, expert_up), scratch=[pltpu.VMEM((m, d), bf16)],
    )
    hiddens = [hidden] + [lax.ppermute(hidden, "tp", around(k, ntp)) for k in range(1, ntp)]
    (column,) = call(stack_kernel, [((8, *joined.shape[1:]), bf16)], (after(near, hidden), low, high))
    planes = [column] + [shift(column, 0, k, 0) for k in range(1, 4)]
    blocks = [column, shift(column, 0, 0, 1)]
    (back,) = call(
        down_kernel, [((n_pick, quarter // 2), bf16)], (*hiddens, *downs), in_specs=[VM] * 4 + [HBM] * 4,
        scratch=[pltpu.VMEM((ntp, expert_down.shape[1], quarter), bf16), pltpu.SemaphoreType.DMA((4,))],
    )
    returned = lax.all_to_all(back.reshape(nep, 8, -1), "ep", 0, 0, tiled=True)
    returned = returned.reshape(n_pick, -1)
    for block in planes[1:]:
        blocks += [block, shift(block, 0, 0, 1)]
    shares = call(
        shared_kernel, [((rows, quarter), f32)] + [((rows, quarter), bf16)] * 3,
        (jnp.stack([lax.axis_index("ep"), part[0]]), after(normed_mix, back), shared_down, residual,
         mix_gate, *blocks),
        in_specs=[SM, VM, VM, HBM] + [VM] * 9,
        scratch=[pltpu.VMEM((rows, d), f32), pltpu.VMEM((rows, quarter), f32), pltpu.SemaphoreType.DMA],
    )
    shares = [shares[0]] + [lax.ppermute(shares[k], "tp", around(k, ntp)) for k in range(1, ntp)]
    (layer_out,) = call(
        final_kernel, [((rows, quarter), bf16)],
        (returned, mix, mix_gate, *shares),
    )
    return (layer_out, new_kv)


def solution(mesh):
    placed = (
        P("ep", None), P("ep"), P("ep", None, "tp"), P(), P(None, "tp"), P(None, "tp"), P(None, "tp"),
        P("tp"), P("tp", None), P(), P("ep", None), P("ep", None), P("ep", None, "tp"),
        P("ep", None, "tp"), P("ep", "tp", None), P("ep", "tp"), P("ep", "tp"), P("tp", None), P(),
    )

    return jax.shard_map(shards, mesh=mesh, in_specs=placed, out_specs=(P("ep", "tp"), P("ep", "tp")), check_vma=False)
```

```python
import jax
import jax.numpy as jnp
from jax import lax
from jax.experimental import pallas as pl
from jax.experimental.pallas import tpu as pltpu
from jax.sharding import PartitionSpec as P

HEAD_DIM = 64
EPS = 1e-06
CAP = 3
Z_ORDER = (0, -1, 1, -3, -4, -2, 3, 2)
bf16 = jnp.bfloat16
f32 = jnp.float32

VM = pl.BlockSpec(memory_space=pltpu.VMEM)
SM = pl.BlockSpec(memory_space=pltpu.SMEM)
HBM = pl.BlockSpec(memory_space=pltpu.HBM)


def iota(shape, dim):
    return lax.broadcasted_iota(jnp.int32, shape, dim)


def dot(a, b, dims=((1,), (0,))):
    return lax.dot_general(a, b, (dims, ((), ())), preferred_element_type=f32)


def three_pieces(values):
    high = values.astype(bf16)
    rest = values - high.astype(f32)
    middle = rest.astype(bf16)
    low = (rest - middle.astype(f32)).astype(bf16)
    return high, middle, low


def hbm(value):
    return pltpu.with_memory_space_constraint(value, pltpu.HBM)


def call(kernel, outs, ins, in_specs=None, out_specs=None, scratch=(), limit_mib=8):
    in_specs = in_specs or [VM] * len(ins)
    out_specs = out_specs or [VM] * len(outs)
    ins = [hbm(x) if spec is HBM else x for x, spec in zip(ins, in_specs)]
    shapes = [
        pltpu.HBM(s, t) if spec is HBM else jax.ShapeDtypeStruct(s, t) for (s, t), spec in zip(outs, out_specs)
    ]
    return pl.pallas_call(
        kernel,
        out_shape=tuple(shapes),
        in_specs=in_specs,
        out_specs=tuple(out_specs),
        scratch_shapes=list(scratch),
        compiler_params=pltpu.CompilerParams(vmem_limit_bytes=limit_mib * 1024 * 1024),
    )(*ins)


def copy_all(pairs, sems, first=0):
    copies = [pltpu.make_async_copy(src, dst, sems.at[first + i]) for i, (src, dst) in enumerate(pairs)]
    for c in copies:
        c.start()
    return copies


def attend_kernel(len_hbm, bias_hbm, tok_hbm, gain_hbm, cache_hbm, wq_hbm, wo_hbm, routes_hbm, sg_hbm, su_hbm,
                  part_ref, pick_ref, joined_ref,
                  len_ref, bias_ref, tok_ref, gain_ref, cache_v, wq_v, wo_v, s_v, routes_v, sem_c, sem_w):
    rows = tok_ref.shape[0]
    span = cache_v.shape[1]
    heads = 4
    hr = rows * heads
    small = []
    for i, (src, dst) in enumerate(
        [(tok_hbm, tok_ref), (gain_hbm, gain_ref), (wq_hbm, wq_v), (wo_hbm, wo_v),
         (len_hbm, len_ref), (bias_hbm, bias_ref)]
    ):
        small.append(pltpu.make_async_copy(src, dst, sem_w.at[i]))
    tok_c, gain_c, wq_c, wo_c, len_c, bias_c = small
    routes_c = pltpu.make_async_copy(routes_hbm, routes_v, sem_w.at[6])
    routes_c.start()
    tok_c.start()
    gain_c.start()
    wq_c.start()
    cache_c = []
    for n in range(rows):
        cache_c.append(pltpu.make_async_copy(cache_hbm.at[n], cache_v.at[n], sem_c.at[n]))
    for c in cache_c[:8]:
        c.start()
    len_c.start()
    bias_c.start()
    half = sg_hbm.shape[1]
    joins = copy_all([(sg_hbm, joined_ref.at[0, :, :half]), (su_hbm, joined_ref.at[0, :, half:])], sem_w, 7)
    routes_c.wait()
    make_pick(routes_v, pick_ref)
    tok_c.wait()
    gain_c.wait()
    for c in cache_c[8:12]:
        c.start()
    x = tok_ref[...].astype(f32)
    ms = jnp.mean(x * x, axis=-1, keepdims=True)
    normed = (x * lax.rsqrt(ms + EPS) * gain_ref[...]).astype(bf16)
    expand = (iota((hr, rows), 0) // heads == iota((hr, rows), 1)).astype(bf16)
    lane = iota((hr, heads * HEAD_DIM), 1)
    row = iota((hr, heads * HEAD_DIM), 0)
    fold = ((iota((256, 128), 0) % HEAD_DIM) == iota((256, 128), 1)).astype(bf16)
    wq_c.wait()
    for c in cache_c[12:]:
        c.start()
    wo_c.start()
    q = dot(normed, wq_v[...]).astype(bf16)
    qx = jnp.where(lane // HEAD_DIM == row % heads, dot(expand, q), 0.0).astype(bf16)
    fold4 = ((iota((256, 256), 0) % HEAD_DIM) == (iota((256, 256), 1) % HEAD_DIM)).astype(bf16)
    narrow_q = dot(qx, fold4) * (HEAD_DIM**-0.5)
    narrow_q = jnp.where(lane // HEAD_DIM == (row // heads) % 4, narrow_q, 0.0).astype(bf16)
    for g in range(rows // 4):
        for n in range(4 * g, 4 * g + 4):
            cache_c[n].wait()
        keys = jnp.concatenate([cache_v[n][:, :HEAD_DIM] for n in range(4 * g, 4 * g + 4)], axis=1)
        s_v[16 * g : 16 * g + 16, :] = dot(narrow_q[16 * g : 16 * g + 16, :], keys, ((1,), (1,)))
    rid = iota((hr, 128), 0)
    lens = jnp.zeros((hr, 128), jnp.int32)
    bias = jnp.zeros((hr, 128), f32)
    len_c.wait()
    bias_c.wait()
    for n in range(rows):
        lens = jnp.where(rid // heads == n, len_ref[n], lens)
    for h in range(heads):
        bias = jnp.where(rid % heads == h, bias_ref[h], bias)
    later = ((iota((128, 256), 0) > iota((128, 256), 1)) | (iota((128, 256), 1) >= 128)).astype(bf16)
    blocks = span // 128
    usable, own, pieces = [], [], []
    for b in range(blocks):
        z = s_v[:, b * 128 : (b + 1) * 128] + bias
        ok = (iota((hr, 128), 1) + b * 128) < lens
        soft = jnp.log1p(jnp.exp(-jnp.abs(z)))
        usable.append(ok)
        own.append(jnp.minimum(z, 0.0) - soft)
        pieces.append(three_pieces(jnp.where(ok, -(jnp.maximum(z, 0.0) + soft), 0.0)))
    high, middle, low = [jnp.concatenate([p[i] for p in pieces], axis=0) for i in range(3)]
    both = (dot(low, later) + dot(middle, later)) + dot(high, later)
    beyond = jnp.zeros((hr, 128), f32)
    weights = [None] * blocks
    for b in range(blocks - 1, -1, -1):
        mine = both[b * hr : (b + 1) * hr, :]
        behind = mine[:, :128] + beyond
        beyond = beyond + mine[:, 128:]
        weights[b] = jnp.where(usable[b], jnp.exp(own[b] + behind), 0.0).astype(bf16)
    outs = []
    r16o = iota((16, 128), 0) // heads
    for g in range(rows // 4):
        pg = jnp.concatenate([w[16 * g : 16 * g + 16, :] for w in weights], axis=1)
        acc = None
        for i in range(4):
            o = dot(pg, cache_v[4 * g + i])
            acc = o if acc is None else jnp.where(r16o == i, o, acc)
        outs.append(acc)
    o = jnp.concatenate(outs, axis=0).astype(bf16)
    unfold = ((iota((128, 256), 0) - HEAD_DIM) == (iota((128, 256), 1) % HEAD_DIM)).astype(bf16)
    ox = jnp.where(lane // HEAD_DIM == row % heads, dot(o, unfold), 0.0).astype(bf16)
    collect = (iota((rows, hr), 1) // heads == iota((rows, hr), 0)).astype(bf16)
    heads_out = dot(collect, ox).astype(bf16)
    wo_c.wait()
    part_ref[...] = dot(heads_out, wo_v[...]).astype(bf16)
    for c in joins:
        c.wait()


def attend(tokens, lengths, cache, gain, wq, bias, wo, routes, shared_gate, shared_up):
    rows, d = tokens.shape
    n_pick = 8 * 64
    return call(
        attend_kernel, [((rows, d), bf16), ((n_pick, CAP * 8 * rows), bf16), ((1, shared_gate.shape[0], 256), bf16)],
        (lengths, bias, tokens, gain.reshape(1, -1), cache, wq, wo, routes, shared_gate, shared_up),
        in_specs=[HBM] * 10,
        scratch=[
            pltpu.SMEM(lengths.shape, jnp.int32), pltpu.SMEM(bias.shape, f32),
            pltpu.VMEM(tokens.shape, bf16), pltpu.VMEM((1, d), f32),
            pltpu.VMEM(cache.shape, bf16), pltpu.VMEM(wq.shape, bf16), pltpu.VMEM(wo.shape, bf16),
            pltpu.VMEM((4 * rows, cache.shape[1]), f32), pltpu.VMEM(routes.shape, jnp.int32),
            pltpu.SemaphoreType.DMA((rows,)), pltpu.SemaphoreType.DMA((9,)),
        ],
        limit_mib=16,
    )


def slots_of(routes_ref, rw_ref):
    top, rows = routes_ref.shape
    experts = 64
    hits = jnp.zeros((experts, rows), f32)
    weight = jnp.zeros((experts, rows), f32)
    which = iota((experts, rows), 0)
    for j in range(top):
        same = which == routes_ref[j : j + 1, :]
        hits = jnp.where(same, 1.0, hits)
        if rw_ref is not None:
            weight = jnp.where(same, rw_ref[j : j + 1, :], weight)
    before = (iota((rows, rows), 0) < iota((rows, rows), 1)).astype(bf16)
    rank = dot(hits.astype(bf16), before)
    slots = [jnp.where((hits > 0.5) & (rank == k), 1.0, 0.0) for k in range(CAP)]
    spread = (iota((8 * experts, experts), 0) // 8 == iota((8 * experts, experts), 1)).astype(bf16)
    return slots, weight, spread


def make_pick(routes_ref, pick_ref):
    rows = routes_ref.shape[1]
    slots, _, spread = slots_of(routes_ref, None)
    n = spread.shape[0]
    tile = (iota((rows, 8 * rows), 0) == iota((rows, 8 * rows), 1) % rows).astype(bf16)
    here = (iota((n, 8 * rows), 0) % 8) == (iota((n, 8 * rows), 1) // rows)
    for k in range(CAP):
        wide = dot(slots[k].astype(bf16), tile).astype(bf16)
        full = jnp.where(here, dot(spread, wide), 0.0)
        pick_ref[:, k * 8 * rows : (k + 1) * 8 * rows] = full.astype(bf16)


def mix_kernel(part_ref, tok_ref, p0, p1, p2, p3, gain_ref, pick_ref, normed_hbm, residual_hbm, sent_hbm,
               normed_v, residual_v, sent_v, sems):
    rows, d = tok_ref.shape
    wide = d // 8
    quarter = residual_hbm.shape[1]
    total = (p0[...].astype(f32) + p1[...].astype(f32)) + (p2[...].astype(f32) + p3[...].astype(f32))
    residual = tok_ref[...].astype(f32) + total
    residual_v[...] = residual
    ms = jnp.mean(residual * residual, axis=-1, keepdims=True)
    normed = (residual * lax.rsqrt(ms + EPS) * gain_ref[...]).astype(bf16)
    normed_v[...] = normed
    mine = pl.ds(pl.multiple_of(part_ref[0] * quarter, quarter), quarter)
    copies = copy_all([(normed_v, normed_hbm), (residual_v.at[:, mine], residual_hbm)], sems)
    stacked = jnp.concatenate([normed[:, r * wide : (r + 1) * wide] for r in range(8)], axis=0)
    for k in range(CAP):
        pick = pick_ref[:, k * 8 * rows : (k + 1) * 8 * rows]
        cols = slice(k * wide, (k + 1) * wide)
        sent_v[:, cols] = dot(pick, stacked).astype(bf16)
        copies += copy_all([(sent_v.at[:, cols], sent_hbm.at[:, cols])], sems, 2 + k)
    for c in copies:
        c.wait()


def stack_kernel(near_ref, low_ref, high_ref, out_ref):
    out_ref[0:3] = near_ref[...]
    out_ref[3:6] = low_ref[...]
    out_ref[6:8] = high_ref[0:2]


def cut_kernel(part_ref, down_hbm, o0, o1, o2, o3, all_v, sems):
    outs = (o0, o1, o2, o3)
    quarter = o0.shape[1]
    for c in copy_all([(down_hbm.at[0], all_v)], sems, 4):
        c.wait()
    pairs = []
    for k in (1, 3, 2, 0):
        cols = pl.ds(pl.multiple_of(((part_ref[0] + k) % 4) * quarter, quarter), quarter)
        pairs.append((all_v.at[:, cols], outs[k]))
    for c in copy_all(pairs, sems):
        c.wait()


def silu(v):
    return v / (1.0 + jnp.exp(-v))


def shared_kernel(at_ref, normed_ref, down_ref, residual_hbm, gate_ref, b0, b1, b2, b3, b4, b5, b6, b7,
                  base_ref, o1, o2, o3, all_v, residual_v, sem):
    blocks = (b0, b1, b2, b3, b4, b5, b6, b7)
    rows, d = normed_ref.shape
    wide = d // 8
    fetch = pltpu.make_async_copy(residual_hbm, residual_v, sem)
    fetch.start()
    ep = at_ref[0]
    z = ep // 8
    y = (ep // 2) % 4
    c = ep % 2
    lane = iota((wide, wide), 1)
    there = ((y + 4 - lane // 64) % 4) * 64 + ((c + lane // 32) % 2) * 32 + lane % 32
    order = (iota((wide, wide), 0) == there).astype(bf16)
    cols = [normed_ref[:, pl.ds(pl.multiple_of(((z + 8 + j) % 8) * wide, wide), wide)] for j in Z_ORDER]
    mine = dot(jnp.concatenate(cols, axis=0), order).astype(bf16)
    n = b0.shape[2]
    acc = jnp.zeros((rows, n), f32)
    for j in range(8):
        w = jnp.concatenate([b[j] for b in blocks], axis=0)
        acc = acc + dot(mine[j * rows : (j + 1) * rows, :], w)
    half = n // 2
    hidden = silu(acc[:, :half]) * acc[:, half:]
    all_v[...] = dot(hidden.astype(bf16), down_ref[...])
    quarter = o1.shape[1]
    cols = [pl.ds(pl.multiple_of(((at_ref[1] + k) % 4) * quarter, quarter), quarter) for k in range(4)]
    for k, o in enumerate((o1, o2, o3)):
        o[...] = all_v[:, cols[k + 1]].astype(bf16)
    fetch.wait()
    base_ref[...] = residual_v[...] + gate_ref[:, :1] * all_v[:, cols[0]]


def expert_kernel(arrived_ref, wg_ref, wu_ref, d0, d1, d2, d3, hidden_ref, downs_ref, x_v, sems):
    fetches = copy_all([(w, downs_ref.at[k]) for k, w in enumerate((d0, d1, d2, d3))], sems)
    n = arrived_ref.shape[0]
    peers = n // 8
    wide = arrived_ref.shape[1] // CAP
    a = iota((n, n), 0)
    b = iota((n, n), 1)
    order = ((b // 8 == a % peers) & (b % 8 == a // peers)).astype(bf16)
    sorted_rows = dot(order, arrived_ref[...]).astype(bf16)
    for r in range(8):
        for k in range(CAP):
            x_v[k * peers : (k + 1) * peers, r * wide : (r + 1) * wide] = sorted_rows[
                r * peers : (r + 1) * peers, k * wide : (k + 1) * wide
            ]
    x = x_v[...]
    gate = dot(x, wg_ref[0])
    up = dot(x, wu_ref[0])
    hidden_ref[...] = (silu(gate) * up).astype(bf16)
    for c in fetches:
        c.wait()


def down_kernel(h0, h1, h2, h3, w_ref, back_hbm, back_v, sems):
    n = back_v.shape[0]
    peers = n // 8
    m = CAP * peers
    a = iota((n, 2 * m), 0)
    b = iota((n, 2 * m), 1)
    order = ((a % 8 == b // peers) & (a // 8 == b % peers)).astype(bf16)
    acc = None
    for k, h in enumerate((h0, h1, h2, h3)):
        part = dot(h[...], w_ref[k])
        acc = part if acc is None else acc + part
    out = acc.astype(bf16)
    half = out.shape[1] // 2
    pieces = [
        out[k * peers : (k + 1) * peers, h * half : (h + 1) * half] for k in range(CAP) for h in range(2)
    ]
    rhs = jnp.concatenate(pieces, axis=0)
    sends = []
    for i in range(2):
        at = slice(i * n // 2, (i + 1) * n // 2)
        back_v[at, :] = dot(order[at, :], rhs).astype(bf16)
        sends += copy_all([(back_v.at[at, :], back_hbm.at[at, :])], sems, 4 + i)
    for c in sends:
        c.wait()


def side_kernel(routes_ref, rw_ref, tok_hbm, gain_ref, kw_hbm, vw_hbm, mixed_hbm, gv_ref,
                mix_ref, kv_ref, gate_ref, tok_ref, both_ref, mixed_ref, sems):
    rows = tok_ref.shape[0]
    n = kw_hbm.shape[0]
    copies = copy_all([(tok_hbm, tok_ref), (kw_hbm, both_ref.at[:n, :]), (vw_hbm, both_ref.at[n:, :]),
                       (mixed_hbm, mixed_ref)], sems)
    for c in copies:
        c.wait()
    x = tok_ref[...].astype(f32)
    ms = jnp.mean(x * x, axis=-1, keepdims=True)
    normed = (x * lax.rsqrt(ms + EPS) * gain_ref[...]).astype(bf16)
    kv_ref[...] = dot(normed, both_ref[...], ((1,), (1,))).astype(bf16)
    slots, weight, spread = slots_of(routes_ref, rw_ref)
    lane = iota((rows, spread.shape[0]), 1) % 8
    mixed = [jnp.zeros(lane.shape, f32) for _ in range(3)]
    for k in range(CAP):
        for i, piece in enumerate(three_pieces(slots[k] * weight)):
            mixed[i] = jnp.where(lane // 2 == k, dot(piece, spread, ((0,), (1,))), mixed[i])
    for h in range(2):
        for i in range(3):
            row = (h * 3 + i) * rows
            mix_ref[row : row + rows, :] = jnp.where(lane % 2 == h, mixed[i], 0.0).astype(bf16)
    total = jnp.zeros((rows, 128), f32)
    for j in range(gv_ref.shape[0]):
        total = total + mixed_ref[:, j * 128 : (j + 1) * 128].astype(f32) * gv_ref[j : j + 1, :].astype(f32)
    logit = jnp.sum(total, axis=-1, keepdims=True)
    gate_ref[...] = jnp.broadcast_to(1.0 / (1.0 + jnp.exp(-logit)), gate_ref.shape)


def final_kernel(back_ref, mix_ref, gate_ref, base_ref, s1, s2, s3, out_ref):
    rows = out_ref.shape[0]
    half = out_ref.shape[1] // 2
    shared = s1[...].astype(f32) + (s2[...].astype(f32) + s3[...].astype(f32))
    base = base_ref[...] + gate_ref[:, :1] * shared
    for h in range(2):
        r = dot(mix_ref[h * 3 * rows : (h + 1) * 3 * rows, :], back_ref[...])
        routed = (r[2 * rows :] + r[rows : 2 * rows]) + r[:rows]
        cols = slice(h * half, (h + 1) * half)
        out_ref[:, cols] = (base[:, cols] + routed).astype(bf16)


def around(k, size):
    return [(i, (i + k) % size) for i in range(size)]


def after(value, *deps):
    return lax.optimization_barrier((value, *deps))[0]


def shards(
    tokens, lengths, cache, attn_gain, query_weight, key_weight, value_weight, stick_bias, out_weight,
    ffn_gain, routes, route_weights, expert_gate, expert_up, expert_down, shared_gate, shared_up,
    shared_down, gate_vector,
):
    ntp = lax.axis_size("tp")
    nep = lax.axis_size("ep")
    rows, d = tokens.shape
    quarter = d // ntp
    part = lax.axis_index("tp").reshape(1)
    n_pick = 8 * nep

    def shift(value, dz, dy, dc):
        perm = []
        for i in range(nep):
            z, y, c = i // 8, i // 2 % 4, i % 2
            perm.append((i, (z + dz) % (nep // 8) * 8 + (y + dy) % 4 * 2 + (c + dc) % 2))
        return lax.ppermute(value, "ep", perm)

    partial, pick, joined = attend(
        tokens, lengths, cache, attn_gain, query_weight, stick_bias, out_weight, routes.T, shared_gate, shared_up
    )
    others = [lax.ppermute(partial, "tp", around(k, ntp)) for k in (2, 1, 3)]
    near = [joined, shift(joined, 1, 0, 0), shift(joined, -1, 0, 0)]
    normed_mix, residual, sent = call(
        mix_kernel, [((rows, d), bf16), ((rows, quarter), f32), ((n_pick, CAP * d // 8), bf16)],
        (part, tokens, partial, *others, ffn_gain.reshape(1, -1), pick),
        in_specs=[SM] + [VM] * 7, out_specs=[HBM] * 3,
        scratch=[pltpu.VMEM((rows, d), bf16), pltpu.VMEM((rows, d), f32),
                 pltpu.VMEM((n_pick, CAP * d // 8), bf16), pltpu.SemaphoreType.DMA((5,))],
    )
    arrived = lax.all_to_all(sent.reshape(nep, 8, -1), "ep", 0, 0, tiled=True)
    arrived = arrived.reshape(n_pick, -1)
    near = jnp.concatenate(after(near, sent))
    low, high = shift(near, 3, 0, 0), shift(near, -3, 0, 0)
    f = expert_down.shape[1]
    cuts = call(
        cut_kernel, [((f, quarter), bf16)] * 4, (part, after(expert_down, sent)),
        in_specs=[SM, HBM], out_specs=[HBM] * 4,
        scratch=[pltpu.VMEM((f, d), bf16), pltpu.SemaphoreType.DMA((5,))],
    )
    downs = [cuts[0]] + [lax.ppermute(cuts[k], "tp", around(k, ntp)) for k in range(1, ntp)]
    mix, new_kv, mix_gate = call(
        side_kernel,
        [((6 * rows, n_pick), bf16), ((rows, 2 * HEAD_DIM), bf16), ((rows, 128), f32)],
        (routes.T, route_weights.T, after(tokens, sent), attn_gain.reshape(1, -1), key_weight.T, value_weight.T,
         normed_mix, gate_vector.reshape(-1, 128)),
        in_specs=[VM, VM, HBM, VM, HBM, HBM, HBM, VM],
        scratch=[pltpu.VMEM((rows, d), bf16), pltpu.VMEM((2 * HEAD_DIM, d), bf16), pltpu.VMEM((rows, d), bf16),
                 pltpu.SemaphoreType.DMA((4,))],
    )
    m = CAP * nep
    hidden, downs = call(
        expert_kernel, [((m, f), bf16), ((ntp, f, quarter), bf16)],
        (arrived, expert_gate, expert_up, *downs), in_specs=[VM] * 3 + [HBM] * 4,
        scratch=[pltpu.VMEM((m, d), bf16), pltpu.SemaphoreType.DMA((4,))],
    )
    hiddens = [hidden] + [lax.ppermute(hidden, "tp", around(k, ntp)) for k in range(1, ntp)]
    (column,) = call(stack_kernel, [((8, *joined.shape[1:]), bf16)], (after(near, hidden), low, high))
    planes = [column] + [shift(column, 0, k, 0) for k in range(1, 4)]
    blocks = [column, shift(column, 0, 0, 1)]
    (back,) = call(
        down_kernel, [((n_pick, quarter // 2), bf16)], (*hiddens, downs), out_specs=[HBM],
        scratch=[pltpu.VMEM((n_pick, quarter // 2), bf16), pltpu.SemaphoreType.DMA((6,))],
    )
    returned = lax.all_to_all(back.reshape(nep, 8, -1), "ep", 0, 0, tiled=True)
    returned = returned.reshape(n_pick, -1)
    for block in planes[1:]:
        blocks += [block, shift(block, 0, 0, 1)]
    shares = call(
        shared_kernel, [((rows, quarter), f32)] + [((rows, quarter), bf16)] * 3,
        (jnp.stack([lax.axis_index("ep"), part[0]]), after(normed_mix, back), shared_down, residual,
         mix_gate, *blocks),
        in_specs=[SM, VM, VM, HBM] + [VM] * 9,
        scratch=[pltpu.VMEM((rows, d), f32), pltpu.VMEM((rows, quarter), f32), pltpu.SemaphoreType.DMA],
    )
    shares = [shares[0]] + [lax.ppermute(shares[k], "tp", around(k, ntp)) for k in range(1, ntp)]
    (layer_out,) = call(
        final_kernel, [((rows, quarter), bf16)],
        (returned, mix, mix_gate, *shares),
    )
    return (layer_out, new_kv)


def solution(mesh):
    placed = (
        P("ep", None), P("ep"), P("ep", None, "tp"), P(), P(None, "tp"), P(None, "tp"), P(None, "tp"),
        P("tp"), P("tp", None), P(), P("ep", None), P("ep", None), P("ep", None, "tp"),
        P("ep", None, "tp"), P("ep", "tp", None), P("ep", "tp"), P("ep", "tp"), P("tp", None), P(),
    )

    return jax.shard_map(shards, mesh=mesh, in_specs=placed, out_specs=(P("ep", "tp"), P("ep", "tp")), check_vma=False)
```

```python
import jax
import jax.numpy as jnp
from jax import lax
from jax.experimental import pallas as pl
from jax.experimental.pallas import tpu as pltpu
from jax.sharding import PartitionSpec as P

HEAD_DIM = 64
EPS = 1e-06
CAP = 3
Z_ORDER = (0, -1, -2, -3, -4, -5, 2, 1)
bf16 = jnp.bfloat16
f32 = jnp.float32

VM = pl.BlockSpec(memory_space=pltpu.VMEM)
SM = pl.BlockSpec(memory_space=pltpu.SMEM)
HBM = pl.BlockSpec(memory_space=pltpu.HBM)


def iota(shape, dim):
    return lax.broadcasted_iota(jnp.int32, shape, dim)


def dot(a, b, dims=((1,), (0,))):
    return lax.dot_general(a, b, (dims, ((), ())), preferred_element_type=f32)


def three_pieces(values):
    high = values.astype(bf16)
    rest = values - high.astype(f32)
    middle = rest.astype(bf16)
    low = (rest - middle.astype(f32)).astype(bf16)
    return high, middle, low


def hbm(value):
    return pltpu.with_memory_space_constraint(value, pltpu.HBM)


def call(kernel, outs, ins, in_specs=None, out_specs=None, scratch=(), limit_mib=8):
    in_specs = in_specs or [VM] * len(ins)
    out_specs = out_specs or [VM] * len(outs)
    ins = [hbm(x) if spec is HBM else x for x, spec in zip(ins, in_specs)]
    shapes = [
        pltpu.HBM(s, t) if spec is HBM else jax.ShapeDtypeStruct(s, t) for (s, t), spec in zip(outs, out_specs)
    ]
    return pl.pallas_call(
        kernel,
        out_shape=tuple(shapes),
        in_specs=in_specs,
        out_specs=tuple(out_specs),
        scratch_shapes=list(scratch),
        compiler_params=pltpu.CompilerParams(vmem_limit_bytes=limit_mib * 1024 * 1024),
    )(*ins)


def copy_all(pairs, sems, first=0):
    copies = [pltpu.make_async_copy(src, dst, sems.at[first + i]) for i, (src, dst) in enumerate(pairs)]
    for c in copies:
        c.start()
    return copies


def attend_kernel(len_hbm, bias_hbm, tok_hbm, gain_hbm, cache_hbm, wq_hbm, wo_hbm, routes_hbm, sg_hbm, su_hbm,
                  part_ref, pick_ref, joined_ref,
                  len_ref, bias_ref, tok_ref, gain_ref, cache_v, wq_v, wo_v, s_v, routes_v, sem_c, sem_w):
    rows = tok_ref.shape[0]
    span = cache_v.shape[1]
    heads = 4
    hr = rows * heads
    small = []
    for i, (src, dst) in enumerate(
        [(tok_hbm, tok_ref), (gain_hbm, gain_ref), (wq_hbm, wq_v), (wo_hbm, wo_v),
         (len_hbm, len_ref), (bias_hbm, bias_ref)]
    ):
        small.append(pltpu.make_async_copy(src, dst, sem_w.at[i]))
    tok_c, gain_c, wq_c, wo_c, len_c, bias_c = small
    routes_c = pltpu.make_async_copy(routes_hbm, routes_v, sem_w.at[6])
    routes_c.start()
    tok_c.start()
    gain_c.start()
    wq_c.start()
    cache_c = []
    for n in range(rows):
        cache_c.append(pltpu.make_async_copy(cache_hbm.at[n], cache_v.at[n], sem_c.at[n]))
    for c in cache_c[:8]:
        c.start()
    len_c.start()
    bias_c.start()
    half = sg_hbm.shape[1]
    joins = copy_all([(sg_hbm, joined_ref.at[0, :, :half]), (su_hbm, joined_ref.at[0, :, half:])], sem_w, 7)
    routes_c.wait()
    make_pick(routes_v, pick_ref)
    tok_c.wait()
    gain_c.wait()
    for c in cache_c[8:12]:
        c.start()
    x = tok_ref[...].astype(f32)
    ms = jnp.mean(x * x, axis=-1, keepdims=True)
    normed = (x * lax.rsqrt(ms + EPS) * gain_ref[...]).astype(bf16)
    expand = (iota((hr, rows), 0) // heads == iota((hr, rows), 1)).astype(bf16)
    lane = iota((hr, heads * HEAD_DIM), 1)
    row = iota((hr, heads * HEAD_DIM), 0)
    fold = ((iota((256, 128), 0) % HEAD_DIM) == iota((256, 128), 1)).astype(bf16)
    wq_c.wait()
    for c in cache_c[12:]:
        c.start()
    wo_c.start()
    q = dot(normed, wq_v[...]).astype(bf16)
    qx = jnp.where(lane // HEAD_DIM == row % heads, dot(expand, q), 0.0).astype(bf16)
    fold4 = ((iota((256, 256), 0) % HEAD_DIM) == (iota((256, 256), 1) % HEAD_DIM)).astype(bf16)
    narrow_q = dot(qx, fold4) * (HEAD_DIM**-0.5)
    narrow_q = jnp.where(lane // HEAD_DIM == (row // heads) % 4, narrow_q, 0.0).astype(bf16)
    for g in range(rows // 4):
        for n in range(4 * g, 4 * g + 4):
            cache_c[n].wait()
        keys = jnp.concatenate([cache_v[n][:, :HEAD_DIM] for n in range(4 * g, 4 * g + 4)], axis=1)
        s_v[16 * g : 16 * g + 16, :] = dot(narrow_q[16 * g : 16 * g + 16, :], keys, ((1,), (1,)))
    rid = iota((hr, 128), 0)
    lens = jnp.zeros((hr, 128), jnp.int32)
    bias = jnp.zeros((hr, 128), f32)
    len_c.wait()
    bias_c.wait()
    for n in range(rows):
        lens = jnp.where(rid // heads == n, len_ref[n], lens)
    for h in range(heads):
        bias = jnp.where(rid % heads == h, bias_ref[h], bias)
    later = ((iota((128, 256), 0) > iota((128, 256), 1)) | (iota((128, 256), 1) >= 128)).astype(bf16)
    blocks = span // 128
    usable, own, pieces = [], [], []
    for b in range(blocks):
        z = s_v[:, b * 128 : (b + 1) * 128] + bias
        ok = (iota((hr, 128), 1) + b * 128) < lens
        soft = jnp.log1p(jnp.exp(-jnp.abs(z)))
        usable.append(ok)
        own.append(jnp.minimum(z, 0.0) - soft)
        pieces.append(three_pieces(jnp.where(ok, -(jnp.maximum(z, 0.0) + soft), 0.0)))
    high, middle, low = [jnp.concatenate([p[i] for p in pieces], axis=0) for i in range(3)]
    both = (dot(low, later) + dot(middle, later)) + dot(high, later)
    beyond = jnp.zeros((hr, 128), f32)
    weights = [None] * blocks
    for b in range(blocks - 1, -1, -1):
        mine = both[b * hr : (b + 1) * hr, :]
        behind = mine[:, :128] + beyond
        beyond = beyond + mine[:, 128:]
        weights[b] = jnp.where(usable[b], jnp.exp(own[b] + behind), 0.0).astype(bf16)
    outs = []
    r16o = iota((16, 128), 0) // heads
    for g in range(rows // 4):
        pg = jnp.concatenate([w[16 * g : 16 * g + 16, :] for w in weights], axis=1)
        acc = None
        for i in range(4):
            o = dot(pg, cache_v[4 * g + i])
            acc = o if acc is None else jnp.where(r16o == i, o, acc)
        outs.append(acc)
    o = jnp.concatenate(outs, axis=0).astype(bf16)
    unfold = ((iota((128, 256), 0) - HEAD_DIM) == (iota((128, 256), 1) % HEAD_DIM)).astype(bf16)
    ox = jnp.where(lane // HEAD_DIM == row % heads, dot(o, unfold), 0.0).astype(bf16)
    collect = (iota((rows, hr), 1) // heads == iota((rows, hr), 0)).astype(bf16)
    heads_out = dot(collect, ox).astype(bf16)
    wo_c.wait()
    part_ref[...] = dot(heads_out, wo_v[...]).astype(bf16)
    for c in joins:
        c.wait()


def attend(tokens, lengths, cache, gain, wq, bias, wo, routes, shared_gate, shared_up):
    rows, d = tokens.shape
    n_pick = 8 * 64
    return call(
        attend_kernel, [((rows, d), bf16), ((n_pick, CAP * 8 * rows), bf16), ((1, shared_gate.shape[0], 256), bf16)],
        (lengths, bias, tokens, gain.reshape(1, -1), cache, wq, wo, routes, shared_gate, shared_up),
        in_specs=[HBM] * 10,
        scratch=[
            pltpu.SMEM(lengths.shape, jnp.int32), pltpu.SMEM(bias.shape, f32),
            pltpu.VMEM(tokens.shape, bf16), pltpu.VMEM((1, d), f32),
            pltpu.VMEM(cache.shape, bf16), pltpu.VMEM(wq.shape, bf16), pltpu.VMEM(wo.shape, bf16),
            pltpu.VMEM((4 * rows, cache.shape[1]), f32), pltpu.VMEM(routes.shape, jnp.int32),
            pltpu.SemaphoreType.DMA((rows,)), pltpu.SemaphoreType.DMA((9,)),
        ],
        limit_mib=16,
    )


def slots_of(routes_ref, rw_ref):
    top, rows = routes_ref.shape
    experts = 64
    hits = jnp.zeros((experts, rows), f32)
    weight = jnp.zeros((experts, rows), f32)
    which = iota((experts, rows), 0)
    for j in range(top):
        same = which == routes_ref[j : j + 1, :]
        hits = jnp.where(same, 1.0, hits)
        if rw_ref is not None:
            weight = jnp.where(same, rw_ref[j : j + 1, :], weight)
    before = (iota((rows, rows), 0) < iota((rows, rows), 1)).astype(bf16)
    rank = dot(hits.astype(bf16), before)
    slots = [jnp.where((hits > 0.5) & (rank == k), 1.0, 0.0) for k in range(CAP)]
    spread = (iota((8 * experts, experts), 0) // 8 == iota((8 * experts, experts), 1)).astype(bf16)
    return slots, weight, spread


def make_pick(routes_ref, pick_ref):
    rows = routes_ref.shape[1]
    slots, _, spread = slots_of(routes_ref, None)
    n = spread.shape[0]
    tile = (iota((rows, 8 * rows), 0) == iota((rows, 8 * rows), 1) % rows).astype(bf16)
    here = (iota((n, 8 * rows), 0) % 8) == (iota((n, 8 * rows), 1) // rows)
    for k in range(CAP):
        wide = dot(slots[k].astype(bf16), tile).astype(bf16)
        full = jnp.where(here, dot(spread, wide), 0.0)
        pick_ref[:, k * 8 * rows : (k + 1) * 8 * rows] = full.astype(bf16)


def mix_kernel(part_ref, tok_ref, p0, p1, p2, p3, gain_ref, pick_ref, normed_hbm, residual_hbm, sent_hbm,
               normed_v, residual_v, sent_v, sems):
    rows, d = tok_ref.shape
    wide = d // 8
    quarter = residual_hbm.shape[1]
    total = (p0[...].astype(f32) + p1[...].astype(f32)) + (p2[...].astype(f32) + p3[...].astype(f32))
    residual = tok_ref[...].astype(f32) + total
    residual_v[...] = residual
    ms = jnp.mean(residual * residual, axis=-1, keepdims=True)
    normed = (residual * lax.rsqrt(ms + EPS) * gain_ref[...]).astype(bf16)
    normed_v[...] = normed
    mine = pl.ds(pl.multiple_of(part_ref[0] * quarter, quarter), quarter)
    copies = copy_all([(normed_v, normed_hbm), (residual_v.at[:, mine], residual_hbm)], sems)
    stacked = jnp.concatenate([normed[:, r * wide : (r + 1) * wide] for r in range(8)], axis=0)
    for k in range(CAP):
        pick = pick_ref[:, k * 8 * rows : (k + 1) * 8 * rows]
        cols = slice(k * wide, (k + 1) * wide)
        sent_v[:, cols] = dot(pick, stacked).astype(bf16)
        copies += copy_all([(sent_v.at[:, cols], sent_hbm.at[:, cols])], sems, 2 + k)
    for c in copies:
        c.wait()


def stack_kernel(r0, r1, r2, r3, out_ref):
    for i, r in enumerate((r0, r1, r2, r3)):
        out_ref[2 * i : 2 * i + 2] = r[...]


def cut_kernel(part_ref, down_hbm, o0, o1, o2, o3, all_v, sems):
    outs = (o0, o1, o2, o3)
    quarter = o0.shape[1]
    for c in copy_all([(down_hbm.at[0], all_v)], sems, 4):
        c.wait()
    pairs = []
    for k in (1, 3, 2, 0):
        cols = pl.ds(pl.multiple_of(((part_ref[0] + k) % 4) * quarter, quarter), quarter)
        pairs.append((all_v.at[:, cols], outs[k]))
    for c in copy_all(pairs, sems):
        c.wait()


def silu(v):
    return v / (1.0 + jnp.exp(-v))


def shared_kernel(at_ref, normed_ref, down_ref, residual_hbm, gate_ref, b0, b1, b2, b3, b4, b5, b6, b7,
                  base_ref, o1, o2, o3, all_v, residual_v, sem):
    blocks = (b0, b1, b2, b3, b4, b5, b6, b7)
    rows, d = normed_ref.shape
    wide = d // 8
    fetch = pltpu.make_async_copy(residual_hbm, residual_v, sem)
    fetch.start()
    ep = at_ref[0]
    z = ep // 8
    y = (ep // 2) % 4
    c = ep % 2
    lane = iota((wide, wide), 1)
    there = ((y + 4 - lane // 64) % 4) * 64 + ((c + lane // 32) % 2) * 32 + lane % 32
    order = (iota((wide, wide), 0) == there).astype(bf16)
    cols = [normed_ref[:, pl.ds(pl.multiple_of(((z + 8 + j) % 8) * wide, wide), wide)] for j in Z_ORDER]
    mine = dot(jnp.concatenate(cols, axis=0), order).astype(bf16)
    n = b0.shape[2]
    acc = jnp.zeros((rows, n), f32)
    for j in range(8):
        w = jnp.concatenate([b[j] for b in blocks], axis=0)
        acc = acc + dot(mine[j * rows : (j + 1) * rows, :], w)
    half = n // 2
    hidden = silu(acc[:, :half]) * acc[:, half:]
    all_v[...] = dot(hidden.astype(bf16), down_ref[...])
    quarter = o1.shape[1]
    cols = [pl.ds(pl.multiple_of(((at_ref[1] + k) % 4) * quarter, quarter), quarter) for k in range(4)]
    for k, o in enumerate((o1, o2, o3)):
        o[...] = all_v[:, cols[k + 1]].astype(bf16)
    fetch.wait()
    base_ref[...] = residual_v[...] + gate_ref[:, :1] * all_v[:, cols[0]]


def expert_kernel(arrived_ref, wg_ref, wu_ref, d0, d1, d2, d3, hidden_ref, downs_ref, x_v, sems):
    fetches = copy_all([(w, downs_ref.at[k]) for k, w in enumerate((d0, d1, d2, d3))], sems)
    n = arrived_ref.shape[0]
    peers = n // 8
    wide = arrived_ref.shape[1] // CAP
    a = iota((n, n), 0)
    b = iota((n, n), 1)
    order = ((b // 8 == a % peers) & (b % 8 == a // peers)).astype(bf16)
    sorted_rows = dot(order, arrived_ref[...]).astype(bf16)
    for r in range(8):
        for k in range(CAP):
            x_v[k * peers : (k + 1) * peers, r * wide : (r + 1) * wide] = sorted_rows[
                r * peers : (r + 1) * peers, k * wide : (k + 1) * wide
            ]
    x = x_v[...]
    gate = dot(x, wg_ref[0])
    up = dot(x, wu_ref[0])
    hidden_ref[...] = (silu(gate) * up).astype(bf16)
    for c in fetches:
        c.wait()


def down_kernel(h0, h1, h2, h3, w_ref, back_hbm, back_v, sems):
    n = back_v.shape[0]
    peers = n // 8
    m = CAP * peers
    a = iota((n, 2 * m), 0)
    b = iota((n, 2 * m), 1)
    order = ((a % 8 == b // peers) & (a // 8 == b % peers)).astype(bf16)
    acc = None
    for k, h in enumerate((h0, h1, h2, h3)):
        part = dot(h[...], w_ref[k])
        acc = part if acc is None else acc + part
    out = acc.astype(bf16)
    half = out.shape[1] // 2
    pieces = [
        out[k * peers : (k + 1) * peers, h * half : (h + 1) * half] for k in range(CAP) for h in range(2)
    ]
    rhs = jnp.concatenate(pieces, axis=0)
    sends = []
    for i in range(2):
        at = slice(i * n // 2, (i + 1) * n // 2)
        back_v[at, :] = dot(order[at, :], rhs).astype(bf16)
        sends += copy_all([(back_v.at[at, :], back_hbm.at[at, :])], sems, 4 + i)
    for c in sends:
        c.wait()


def side_kernel(routes_ref, rw_ref, tok_hbm, gain_ref, kw_hbm, vw_hbm, mixed_hbm, gv_ref,
                mix_ref, kv_ref, gate_ref, tok_ref, both_ref, mixed_ref, sems):
    rows = tok_ref.shape[0]
    n = kw_hbm.shape[0]
    copies = copy_all([(tok_hbm, tok_ref), (kw_hbm, both_ref.at[:n, :]), (vw_hbm, both_ref.at[n:, :]),
                       (mixed_hbm, mixed_ref)], sems)
    for c in copies:
        c.wait()
    x = tok_ref[...].astype(f32)
    ms = jnp.mean(x * x, axis=-1, keepdims=True)
    normed = (x * lax.rsqrt(ms + EPS) * gain_ref[...]).astype(bf16)
    kv_ref[...] = dot(normed, both_ref[...], ((1,), (1,))).astype(bf16)
    slots, weight, spread = slots_of(routes_ref, rw_ref)
    lane = iota((rows, spread.shape[0]), 1) % 8
    mixed = [jnp.zeros(lane.shape, f32) for _ in range(3)]
    for k in range(CAP):
        for i, piece in enumerate(three_pieces(slots[k] * weight)):
            mixed[i] = jnp.where(lane // 2 == k, dot(piece, spread, ((0,), (1,))), mixed[i])
    for h in range(2):
        for i in range(3):
            row = (h * 3 + i) * rows
            mix_ref[row : row + rows, :] = jnp.where(lane % 2 == h, mixed[i], 0.0).astype(bf16)
    total = jnp.zeros((rows, 128), f32)
    for j in range(gv_ref.shape[0]):
        total = total + mixed_ref[:, j * 128 : (j + 1) * 128].astype(f32) * gv_ref[j : j + 1, :].astype(f32)
    logit = jnp.sum(total, axis=-1, keepdims=True)
    gate_ref[...] = jnp.broadcast_to(1.0 / (1.0 + jnp.exp(-logit)), gate_ref.shape)


def final_kernel(back_ref, mix_ref, gate_ref, base_ref, s1, s2, s3, out_ref):
    rows = out_ref.shape[0]
    half = out_ref.shape[1] // 2
    shared = s1[...].astype(f32) + (s2[...].astype(f32) + s3[...].astype(f32))
    base = base_ref[...] + gate_ref[:, :1] * shared
    for h in range(2):
        r = dot(mix_ref[h * 3 * rows : (h + 1) * 3 * rows, :], back_ref[...])
        routed = (r[2 * rows :] + r[rows : 2 * rows]) + r[:rows]
        cols = slice(h * half, (h + 1) * half)
        out_ref[:, cols] = (base[:, cols] + routed).astype(bf16)


def around(k, size):
    return [(i, (i + k) % size) for i in range(size)]


def after(value, *deps):
    return lax.optimization_barrier((value, *deps))[0]


def shards(
    tokens, lengths, cache, attn_gain, query_weight, key_weight, value_weight, stick_bias, out_weight,
    ffn_gain, routes, route_weights, expert_gate, expert_up, expert_down, shared_gate, shared_up,
    shared_down, gate_vector,
):
    ntp = lax.axis_size("tp")
    nep = lax.axis_size("ep")
    rows, d = tokens.shape
    quarter = d // ntp
    part = lax.axis_index("tp").reshape(1)
    n_pick = 8 * nep

    def shift(value, dz, dy, dc):
        perm = []
        for i in range(nep):
            z, y, c = i // 8, i // 2 % 4, i % 2
            perm.append((i, (z + dz) % (nep // 8) * 8 + (y + dy) % 4 * 2 + (c + dc) % 2))
        return lax.ppermute(value, "ep", perm)

    partial, pick, joined = attend(
        tokens, lengths, cache, attn_gain, query_weight, stick_bias, out_weight, routes.T, shared_gate, shared_up
    )
    others = [lax.ppermute(partial, "tp", around(2, ntp))]
    others += [lax.ppermute(partial, "tp", around(k, ntp)) for k in (1, 3)]
    near = [joined, shift(joined, 1, 0, 0)]
    normed_mix, residual, sent = call(
        mix_kernel, [((rows, d), bf16), ((rows, quarter), f32), ((n_pick, CAP * d // 8), bf16)],
        (part, tokens, partial, *others, ffn_gain.reshape(1, -1), pick),
        in_specs=[SM] + [VM] * 7, out_specs=[HBM] * 3,
        scratch=[pltpu.VMEM((rows, d), bf16), pltpu.VMEM((rows, d), f32),
                 pltpu.VMEM((n_pick, CAP * d // 8), bf16), pltpu.SemaphoreType.DMA((5,))],
    )
    arrived = lax.all_to_all(sent.reshape(nep, 8, -1), "ep", 0, 0, tiled=True)
    arrived = arrived.reshape(n_pick, -1)
    near = jnp.concatenate(after(near, sent))
    far = [shift(near, k, 0, 0) for k in (2, 4, -2)]
    f = expert_down.shape[1]
    cuts = call(
        cut_kernel, [((f, quarter), bf16)] * 4, (part, after(expert_down, sent)),
        in_specs=[SM, HBM], out_specs=[HBM] * 4,
        scratch=[pltpu.VMEM((f, d), bf16), pltpu.SemaphoreType.DMA((5,))],
    )
    downs = [cuts[0]] + [lax.ppermute(cuts[k], "tp", around(k, ntp)) for k in range(1, ntp)]
    mix, new_kv, mix_gate = call(
        side_kernel,
        [((6 * rows, n_pick), bf16), ((rows, 2 * HEAD_DIM), bf16), ((rows, 128), f32)],
        (routes.T, route_weights.T, after(tokens, sent), attn_gain.reshape(1, -1), key_weight.T, value_weight.T,
         normed_mix, gate_vector.reshape(-1, 128)),
        in_specs=[VM, VM, HBM, VM, HBM, HBM, HBM, VM],
        scratch=[pltpu.VMEM((rows, d), bf16), pltpu.VMEM((2 * HEAD_DIM, d), bf16), pltpu.VMEM((rows, d), bf16),
                 pltpu.SemaphoreType.DMA((4,))],
    )
    m = CAP * nep
    hidden, downs = call(
        expert_kernel, [((m, f), bf16), ((ntp, f, quarter), bf16)],
        (arrived, expert_gate, expert_up, *downs), in_specs=[VM] * 3 + [HBM] * 4,
        scratch=[pltpu.VMEM((m, d), bf16), pltpu.SemaphoreType.DMA((4,))],
    )
    hiddens = [hidden] + [lax.ppermute(hidden, "tp", around(k, ntp)) for k in range(1, ntp)]
    (column,) = call(stack_kernel, [((8, *joined.shape[1:]), bf16)], (after(near, hidden), *far))
    planes = [column] + [shift(column, 0, k, 0) for k in range(1, 4)]
    blocks = [column, shift(column, 0, 0, 1)]
    (back,) = call(
        down_kernel, [((n_pick, quarter // 2), bf16)], (*hiddens, downs), out_specs=[HBM],
        scratch=[pltpu.VMEM((n_pick, quarter // 2), bf16), pltpu.SemaphoreType.DMA((6,))],
    )
    returned = lax.all_to_all(back.reshape(nep, 8, -1), "ep", 0, 0, tiled=True)
    returned = returned.reshape(n_pick, -1)
    for block in planes[1:]:
        blocks += [block, shift(block, 0, 0, 1)]
    shares = call(
        shared_kernel, [((rows, quarter), f32)] + [((rows, quarter), bf16)] * 3,
        (jnp.stack([lax.axis_index("ep"), part[0]]), after(normed_mix, back), shared_down, residual,
         mix_gate, *blocks),
        in_specs=[SM, VM, VM, HBM] + [VM] * 9,
        scratch=[pltpu.VMEM((rows, d), f32), pltpu.VMEM((rows, quarter), f32), pltpu.SemaphoreType.DMA],
    )
    far_share = lax.ppermute(shares[2], "tp", around(2, ntp))
    shares = [shares[0], far_share] + [lax.ppermute(shares[k], "tp", around(k, ntp)) for k in (1, 3)]
    (layer_out,) = call(
        final_kernel, [((rows, quarter), bf16)],
        (returned, mix, mix_gate, *shares),
    )
    return (layer_out, new_kv)


def solution(mesh):
    placed = (
        P("ep", None), P("ep"), P("ep", None, "tp"), P(), P(None, "tp"), P(None, "tp"), P(None, "tp"),
        P("tp"), P("tp", None), P(), P("ep", None), P("ep", None), P("ep", None, "tp"),
        P("ep", None, "tp"), P("ep", "tp", None), P("ep", "tp"), P("ep", "tp"), P("tp", None), P(),
    )

    return jax.shard_map(shards, mesh=mesh, in_specs=placed, out_specs=(P("ep", "tp"), P("ep", "tp")), check_vma=False)
```

```python
import jax
import jax.numpy as jnp
from jax import lax
from jax.experimental import pallas as pl
from jax.experimental.pallas import tpu as pltpu
from jax.sharding import PartitionSpec as P

HEAD_DIM = 64
EPS = 1e-06
CAP = 3
Z_ORDER = (0, -1, -2, -3, -4, -5, 2, 1)
bf16 = jnp.bfloat16
f32 = jnp.float32

VM = pl.BlockSpec(memory_space=pltpu.VMEM)
SM = pl.BlockSpec(memory_space=pltpu.SMEM)
HBM = pl.BlockSpec(memory_space=pltpu.HBM)


def iota(shape, dim):
    return lax.broadcasted_iota(jnp.int32, shape, dim)


def dot(a, b, dims=((1,), (0,))):
    return lax.dot_general(a, b, (dims, ((), ())), preferred_element_type=f32)


def three_pieces(values):
    high = values.astype(bf16)
    rest = values - high.astype(f32)
    middle = rest.astype(bf16)
    low = (rest - middle.astype(f32)).astype(bf16)
    return high, middle, low


def hbm(value):
    return pltpu.with_memory_space_constraint(value, pltpu.HBM)


def call(kernel, outs, ins, in_specs=None, out_specs=None, scratch=(), limit_mib=8):
    in_specs = in_specs or [VM] * len(ins)
    out_specs = out_specs or [VM] * len(outs)
    ins = [hbm(x) if spec is HBM else x for x, spec in zip(ins, in_specs)]
    shapes = [
        pltpu.HBM(s, t) if spec is HBM else jax.ShapeDtypeStruct(s, t) for (s, t), spec in zip(outs, out_specs)
    ]
    return pl.pallas_call(
        kernel,
        out_shape=tuple(shapes),
        in_specs=in_specs,
        out_specs=tuple(out_specs),
        scratch_shapes=list(scratch),
        compiler_params=pltpu.CompilerParams(vmem_limit_bytes=limit_mib * 1024 * 1024),
    )(*ins)


def copy_all(pairs, sems, first=0):
    copies = [pltpu.make_async_copy(src, dst, sems.at[first + i]) for i, (src, dst) in enumerate(pairs)]
    for c in copies:
        c.start()
    return copies


def attend_kernel(len_hbm, bias_hbm, tok_hbm, gain_hbm, cache_hbm, wq_hbm, wo_hbm, routes_hbm, sg_hbm, su_hbm,
                  part_ref, pick_ref, joined_ref,
                  len_ref, bias_ref, tok_ref, gain_ref, cache_v, wq_v, wo_v, s_v, routes_v, sem_c, sem_w):
    rows = tok_ref.shape[0]
    span = cache_v.shape[1]
    heads = 4
    hr = rows * heads
    small = []
    for i, (src, dst) in enumerate(
        [(tok_hbm, tok_ref), (gain_hbm, gain_ref), (wq_hbm, wq_v), (wo_hbm, wo_v),
         (len_hbm, len_ref), (bias_hbm, bias_ref)]
    ):
        small.append(pltpu.make_async_copy(src, dst, sem_w.at[i]))
    tok_c, gain_c, wq_c, wo_c, len_c, bias_c = small
    routes_c = pltpu.make_async_copy(routes_hbm, routes_v, sem_w.at[6])
    routes_c.start()
    tok_c.start()
    gain_c.start()
    wq_c.start()
    cache_c = []
    for n in range(rows):
        cache_c.append(pltpu.make_async_copy(cache_hbm.at[n], cache_v.at[n], sem_c.at[n]))
    for c in cache_c[:8]:
        c.start()
    len_c.start()
    bias_c.start()
    half = sg_hbm.shape[1]
    joins = copy_all([(sg_hbm, joined_ref.at[0, :, :half]), (su_hbm, joined_ref.at[0, :, half:])], sem_w, 7)
    routes_c.wait()
    make_pick(routes_v, pick_ref)
    tok_c.wait()
    gain_c.wait()
    for c in cache_c[8:12]:
        c.start()
    x = tok_ref[...].astype(f32)
    ms = jnp.mean(x * x, axis=-1, keepdims=True)
    normed = (x * lax.rsqrt(ms + EPS) * gain_ref[...]).astype(bf16)
    expand = (iota((hr, rows), 0) // heads == iota((hr, rows), 1)).astype(bf16)
    lane = iota((hr, heads * HEAD_DIM), 1)
    row = iota((hr, heads * HEAD_DIM), 0)
    fold = ((iota((256, 128), 0) % HEAD_DIM) == iota((256, 128), 1)).astype(bf16)
    wq_c.wait()
    for c in cache_c[12:]:
        c.start()
    wo_c.start()
    q = dot(normed, wq_v[...]).astype(bf16)
    qx = jnp.where(lane // HEAD_DIM == row % heads, dot(expand, q), 0.0).astype(bf16)
    fold4 = ((iota((256, 256), 0) % HEAD_DIM) == (iota((256, 256), 1) % HEAD_DIM)).astype(bf16)
    narrow_q = dot(qx, fold4) * (HEAD_DIM**-0.5)
    narrow_q = jnp.where(lane // HEAD_DIM == (row // heads) % 4, narrow_q, 0.0).astype(bf16)
    for g in range(rows // 4):
        for n in range(4 * g, 4 * g + 4):
            cache_c[n].wait()
        keys = jnp.concatenate([cache_v[n][:, :HEAD_DIM] for n in range(4 * g, 4 * g + 4)], axis=1)
        s_v[16 * g : 16 * g + 16, :] = dot(narrow_q[16 * g : 16 * g + 16, :], keys, ((1,), (1,)))
    rid = iota((hr, 128), 0)
    lens = jnp.zeros((hr, 128), jnp.int32)
    bias = jnp.zeros((hr, 128), f32)
    len_c.wait()
    bias_c.wait()
    for n in range(rows):
        lens = jnp.where(rid // heads == n, len_ref[n], lens)
    for h in range(heads):
        bias = jnp.where(rid % heads == h, bias_ref[h], bias)
    later = ((iota((128, 256), 0) > iota((128, 256), 1)) | (iota((128, 256), 1) >= 128)).astype(bf16)
    blocks = span // 128
    usable, own, pieces = [], [], []
    for b in range(blocks):
        z = s_v[:, b * 128 : (b + 1) * 128] + bias
        ok = (iota((hr, 128), 1) + b * 128) < lens
        soft = jnp.log1p(jnp.exp(-jnp.abs(z)))
        usable.append(ok)
        own.append(jnp.minimum(z, 0.0) - soft)
        pieces.append(three_pieces(jnp.where(ok, -(jnp.maximum(z, 0.0) + soft), 0.0)))
    high, middle, low = [jnp.concatenate([p[i] for p in pieces], axis=0) for i in range(3)]
    both = (dot(low, later) + dot(middle, later)) + dot(high, later)
    beyond = jnp.zeros((hr, 128), f32)
    weights = [None] * blocks
    for b in range(blocks - 1, -1, -1):
        mine = both[b * hr : (b + 1) * hr, :]
        behind = mine[:, :128] + beyond
        beyond = beyond + mine[:, 128:]
        weights[b] = jnp.where(usable[b], jnp.exp(own[b] + behind), 0.0).astype(bf16)
    outs = []
    r16o = iota((16, 128), 0) // heads
    for g in range(rows // 4):
        pg = jnp.concatenate([w[16 * g : 16 * g + 16, :] for w in weights], axis=1)
        acc = None
        for i in range(4):
            o = dot(pg, cache_v[4 * g + i])
            acc = o if acc is None else jnp.where(r16o == i, o, acc)
        outs.append(acc)
    o = jnp.concatenate(outs, axis=0).astype(bf16)
    unfold = ((iota((128, 256), 0) - HEAD_DIM) == (iota((128, 256), 1) % HEAD_DIM)).astype(bf16)
    ox = jnp.where(lane // HEAD_DIM == row % heads, dot(o, unfold), 0.0).astype(bf16)
    collect = (iota((rows, hr), 1) // heads == iota((rows, hr), 0)).astype(bf16)
    heads_out = dot(collect, ox).astype(bf16)
    wo_c.wait()
    part_ref[...] = dot(heads_out, wo_v[...]).astype(bf16)
    for c in joins:
        c.wait()


def attend(tokens, lengths, cache, gain, wq, bias, wo, routes, shared_gate, shared_up):
    rows, d = tokens.shape
    n_pick = 8 * 64
    return call(
        attend_kernel, [((rows, d), bf16), ((n_pick, CAP * 8 * rows), bf16), ((1, shared_gate.shape[0], 256), bf16)],
        (lengths, bias, tokens, gain.reshape(1, -1), cache, wq, wo, routes, shared_gate, shared_up),
        in_specs=[HBM] * 10,
        scratch=[
            pltpu.SMEM(lengths.shape, jnp.int32), pltpu.SMEM(bias.shape, f32),
            pltpu.VMEM(tokens.shape, bf16), pltpu.VMEM((1, d), f32),
            pltpu.VMEM(cache.shape, bf16), pltpu.VMEM(wq.shape, bf16), pltpu.VMEM(wo.shape, bf16),
            pltpu.VMEM((4 * rows, cache.shape[1]), f32), pltpu.VMEM(routes.shape, jnp.int32),
            pltpu.SemaphoreType.DMA((rows,)), pltpu.SemaphoreType.DMA((9,)),
        ],
        limit_mib=16,
    )


def slots_of(routes_ref, rw_ref):
    top, rows = routes_ref.shape
    experts = 64
    hits = jnp.zeros((experts, rows), f32)
    weight = jnp.zeros((experts, rows), f32)
    which = iota((experts, rows), 0)
    for j in range(top):
        same = which == routes_ref[j : j + 1, :]
        hits = jnp.where(same, 1.0, hits)
        if rw_ref is not None:
            weight = jnp.where(same, rw_ref[j : j + 1, :], weight)
    before = (iota((rows, rows), 0) < iota((rows, rows), 1)).astype(bf16)
    rank = dot(hits.astype(bf16), before)
    slots = [jnp.where((hits > 0.5) & (rank == k), 1.0, 0.0) for k in range(CAP)]
    spread = (iota((8 * experts, experts), 0) // 8 == iota((8 * experts, experts), 1)).astype(bf16)
    return slots, weight, spread


def make_pick(routes_ref, pick_ref):
    rows = routes_ref.shape[1]
    slots, _, spread = slots_of(routes_ref, None)
    n = spread.shape[0]
    tile = (iota((rows, 8 * rows), 0) == iota((rows, 8 * rows), 1) % rows).astype(bf16)
    here = (iota((n, 8 * rows), 0) % 8) == (iota((n, 8 * rows), 1) // rows)
    for k in range(CAP):
        wide = dot(slots[k].astype(bf16), tile).astype(bf16)
        full = jnp.where(here, dot(spread, wide), 0.0)
        pick_ref[:, k * 8 * rows : (k + 1) * 8 * rows] = full.astype(bf16)


def mix_kernel(part_ref, tok_ref, p0, p1, p2, p3, gain_ref, pick_ref, normed_hbm, residual_hbm, sent_hbm,
               normed_v, residual_v, sent_v, sems):
    rows, d = tok_ref.shape
    wide = d // 8
    quarter = residual_hbm.shape[1]
    total = (p0[...].astype(f32) + p1[...].astype(f32)) + (p2[...].astype(f32) + p3[...].astype(f32))
    residual = tok_ref[...].astype(f32) + total
    residual_v[...] = residual
    ms = jnp.mean(residual * residual, axis=-1, keepdims=True)
    normed = (residual * lax.rsqrt(ms + EPS) * gain_ref[...]).astype(bf16)
    normed_v[...] = normed
    mine = pl.ds(pl.multiple_of(part_ref[0] * quarter, quarter), quarter)
    copies = copy_all([(normed_v, normed_hbm), (residual_v.at[:, mine], residual_hbm)], sems)
    stacked = jnp.concatenate([normed[:, r * wide : (r + 1) * wide] for r in range(8)], axis=0)
    for k in range(CAP):
        pick = pick_ref[:, k * 8 * rows : (k + 1) * 8 * rows]
        cols = slice(k * wide, (k + 1) * wide)
        sent_v[:, cols] = dot(pick, stacked).astype(bf16)
        copies += copy_all([(sent_v.at[:, cols], sent_hbm.at[:, cols])], sems, 2 + k)
    for c in copies:
        c.wait()


def stack_kernel(r0, r1, r2, r3, out_ref):
    for i, r in enumerate((r0, r1, r2, r3)):
        out_ref[2 * i : 2 * i + 2] = r[...]


def cut_kernel(part_ref, down_hbm, o0, o1, o2, o3, all_v, sems):
    outs = (o0, o1, o2, o3)
    quarter = o0.shape[1]
    for c in copy_all([(down_hbm.at[0], all_v)], sems, 4):
        c.wait()
    pairs = []
    for k in (1, 3, 2, 0):
        cols = pl.ds(pl.multiple_of(((part_ref[0] + k) % 4) * quarter, quarter), quarter)
        pairs.append((all_v.at[:, cols], outs[k]))
    for c in copy_all(pairs, sems):
        c.wait()


def silu(v):
    return v / (1.0 + jnp.exp(-v))


def shared_kernel(at_ref, normed_ref, down_ref, residual_hbm, gate_ref, b0, b1, b2, b3, b4, b5, b6, b7,
                  base_ref, o1, o2, o3, all_v, residual_v, sem):
    blocks = (b0, b1, b2, b3, b4, b5, b6, b7)
    rows, d = normed_ref.shape
    wide = d // 8
    fetch = pltpu.make_async_copy(residual_hbm, residual_v, sem)
    fetch.start()
    ep = at_ref[0]
    z = ep // 8
    y = (ep // 2) % 4
    c = ep % 2
    lane = iota((wide, wide), 1)
    there = ((y + 4 - lane // 64) % 4) * 64 + ((c + lane // 32) % 2) * 32 + lane % 32
    order = (iota((wide, wide), 0) == there).astype(bf16)
    cols = [normed_ref[:, pl.ds(pl.multiple_of(((z + 8 + j) % 8) * wide, wide), wide)] for j in Z_ORDER]
    mine = dot(jnp.concatenate(cols, axis=0), order).astype(bf16)
    n = b0.shape[2]
    acc = jnp.zeros((rows, n), f32)
    for j in range(8):
        w = jnp.concatenate([b[j] for b in blocks], axis=0)
        acc = acc + dot(mine[j * rows : (j + 1) * rows, :], w)
    half = n // 2
    hidden = silu(acc[:, :half]) * acc[:, half:]
    all_v[...] = dot(hidden.astype(bf16), down_ref[...])
    quarter = o1.shape[1]
    cols = [pl.ds(pl.multiple_of(((at_ref[1] + k) % 4) * quarter, quarter), quarter) for k in range(4)]
    for k, o in enumerate((o1, o2, o3)):
        o[...] = all_v[:, cols[k + 1]].astype(bf16)
    fetch.wait()
    base_ref[...] = residual_v[...] + gate_ref[:, :1] * all_v[:, cols[0]]


def expert_kernel(arrived_ref, wg_ref, wu_ref, d0, d1, d2, d3, hidden_ref, downs_ref, x_v, sems):
    fetches = copy_all([(w, downs_ref.at[k]) for k, w in enumerate((d0, d1, d2, d3))], sems)
    n = arrived_ref.shape[0]
    peers = n // 8
    wide = arrived_ref.shape[1] // CAP
    a = iota((n, n), 0)
    b = iota((n, n), 1)
    order = ((b // 8 == a % peers) & (b % 8 == a // peers)).astype(bf16)
    sorted_rows = dot(order, arrived_ref[...]).astype(bf16)
    for r in range(8):
        for k in range(CAP):
            x_v[k * peers : (k + 1) * peers, r * wide : (r + 1) * wide] = sorted_rows[
                r * peers : (r + 1) * peers, k * wide : (k + 1) * wide
            ]
    x = x_v[...]
    gate = dot(x, wg_ref[0])
    up = dot(x, wu_ref[0])
    hidden_ref[...] = (silu(gate) * up).astype(bf16)
    for c in fetches:
        c.wait()


def down_kernel(h0, h1, h2, h3, w_ref, back_hbm, back_v, sems):
    n = back_v.shape[0]
    peers = n // 8
    m = CAP * peers
    a = iota((n, 2 * m), 0)
    b = iota((n, 2 * m), 1)
    order = ((a % 8 == b // peers) & (a // 8 == b % peers)).astype(bf16)
    acc = None
    for k, h in enumerate((h0, h1, h2, h3)):
        part = dot(h[...], w_ref[k])
        acc = part if acc is None else acc + part
    out = acc.astype(bf16)
    half = out.shape[1] // 2
    pieces = [
        out[k * peers : (k + 1) * peers, h * half : (h + 1) * half] for k in range(CAP) for h in range(2)
    ]
    rhs = jnp.concatenate(pieces, axis=0)
    sends = []
    for i in range(2):
        at = slice(i * n // 2, (i + 1) * n // 2)
        back_v[at, :] = dot(order[at, :], rhs).astype(bf16)
        sends += copy_all([(back_v.at[at, :], back_hbm.at[at, :])], sems, 4 + i)
    for c in sends:
        c.wait()


def side_kernel(routes_hbm, rw_hbm, tok_hbm, gain_hbm, kw_hbm, vw_hbm, mixed_hbm, gv_hbm,
                mix_ref, kv_ref, gate_ref, tok_ref, both_ref, mixed_ref, routes_ref, rw_ref, gain_ref, gv_ref, sems):
    rows = tok_ref.shape[0]
    n = kw_hbm.shape[0]
    copies = copy_all([(tok_hbm, tok_ref), (kw_hbm, both_ref.at[:n, :]), (vw_hbm, both_ref.at[n:, :]),
                       (mixed_hbm, mixed_ref), (routes_hbm, routes_ref), (rw_hbm, rw_ref), (gain_hbm, gain_ref),
                       (gv_hbm, gv_ref)], sems)
    for c in copies:
        c.wait()
    x = tok_ref[...].astype(f32)
    ms = jnp.mean(x * x, axis=-1, keepdims=True)
    normed = (x * lax.rsqrt(ms + EPS) * gain_ref[...]).astype(bf16)
    kv_ref[...] = dot(normed, both_ref[...], ((1,), (1,))).astype(bf16)
    slots, weight, spread = slots_of(routes_ref, rw_ref)
    lane = iota((rows, spread.shape[0]), 1) % 8
    mixed = [jnp.zeros(lane.shape, f32) for _ in range(3)]
    for k in range(CAP):
        for i, piece in enumerate(three_pieces(slots[k] * weight)):
            mixed[i] = jnp.where(lane // 2 == k, dot(piece, spread, ((0,), (1,))), mixed[i])
    for h in range(2):
        for i in range(3):
            row = (h * 3 + i) * rows
            mix_ref[row : row + rows, :] = jnp.where(lane % 2 == h, mixed[i], 0.0).astype(bf16)
    total = jnp.zeros((rows, 128), f32)
    for j in range(gv_ref.shape[0]):
        total = total + mixed_ref[:, j * 128 : (j + 1) * 128].astype(f32) * gv_ref[j : j + 1, :].astype(f32)
    logit = jnp.sum(total, axis=-1, keepdims=True)
    gate_ref[...] = jnp.broadcast_to(1.0 / (1.0 + jnp.exp(-logit)), gate_ref.shape)


def final_kernel(back_ref, mix_ref, gate_ref, base_ref, s1, s2, s3, out_ref):
    rows = out_ref.shape[0]
    half = out_ref.shape[1] // 2
    shared = s1[...].astype(f32) + (s2[...].astype(f32) + s3[...].astype(f32))
    base = base_ref[...] + gate_ref[:, :1] * shared
    for h in range(2):
        r = dot(mix_ref[h * 3 * rows : (h + 1) * 3 * rows, :], back_ref[...])
        routed = (r[2 * rows :] + r[rows : 2 * rows]) + r[:rows]
        cols = slice(h * half, (h + 1) * half)
        out_ref[:, cols] = (base[:, cols] + routed).astype(bf16)


def around(k, size):
    return [(i, (i + k) % size) for i in range(size)]


def after(value, *deps):
    return lax.optimization_barrier((value, *deps))[0]


def shards(
    tokens, lengths, cache, attn_gain, query_weight, key_weight, value_weight, stick_bias, out_weight,
    ffn_gain, routes, route_weights, expert_gate, expert_up, expert_down, shared_gate, shared_up,
    shared_down, gate_vector,
):
    ntp = lax.axis_size("tp")
    nep = lax.axis_size("ep")
    rows, d = tokens.shape
    quarter = d // ntp
    part = lax.axis_index("tp").reshape(1)
    n_pick = 8 * nep

    def shift(value, dz, dy, dc):
        perm = []
        for i in range(nep):
            z, y, c = i // 8, i // 2 % 4, i % 2
            perm.append((i, (z + dz) % (nep // 8) * 8 + (y + dy) % 4 * 2 + (c + dc) % 2))
        return lax.ppermute(value, "ep", perm)

    partial, pick, joined = attend(
        tokens, lengths, cache, attn_gain, query_weight, stick_bias, out_weight, routes.T, shared_gate, shared_up
    )
    others = [lax.ppermute(partial, "tp", around(2, ntp))]
    others += [lax.ppermute(partial, "tp", around(k, ntp)) for k in (1, 3)]
    near = [joined, shift(joined, 1, 0, 0)]
    normed_mix, residual, sent = call(
        mix_kernel, [((rows, d), bf16), ((rows, quarter), f32), ((n_pick, CAP * d // 8), bf16)],
        (part, tokens, partial, *others, ffn_gain.reshape(1, -1), pick),
        in_specs=[SM] + [VM] * 7, out_specs=[HBM] * 3,
        scratch=[pltpu.VMEM((rows, d), bf16), pltpu.VMEM((rows, d), f32),
                 pltpu.VMEM((n_pick, CAP * d // 8), bf16), pltpu.SemaphoreType.DMA((5,))],
    )
    arrived = lax.all_to_all(sent.reshape(nep, 8, -1), "ep", 0, 0, tiled=True)
    arrived = arrived.reshape(n_pick, -1)
    near = jnp.concatenate(after(near, sent))
    far = [shift(near, k, 0, 0) for k in (2, 4, -2)]
    f = expert_down.shape[1]
    cuts = call(
        cut_kernel, [((f, quarter), bf16)] * 4, (part, after(expert_down, sent)),
        in_specs=[SM, HBM], out_specs=[HBM] * 4,
        scratch=[pltpu.VMEM((f, d), bf16), pltpu.SemaphoreType.DMA((5,))],
    )
    downs = [cuts[0]] + [lax.ppermute(cuts[k], "tp", around(k, ntp)) for k in range(1, ntp)]
    mix, new_kv, mix_gate = call(
        side_kernel,
        [((6 * rows, n_pick), bf16), ((rows, 2 * HEAD_DIM), bf16), ((rows, 128), f32)],
        (routes.T, route_weights.T, after(tokens, sent), attn_gain.reshape(1, -1), key_weight.T, value_weight.T,
         normed_mix, gate_vector.reshape(-1, 128)),
        in_specs=[HBM] * 8,
        scratch=[pltpu.VMEM((rows, d), bf16), pltpu.VMEM((2 * HEAD_DIM, d), bf16), pltpu.VMEM((rows, d), bf16),
                 pltpu.VMEM(routes.T.shape, jnp.int32), pltpu.VMEM(routes.T.shape, f32), pltpu.VMEM((1, d), f32),
                 pltpu.VMEM((d // 128, 128), bf16), pltpu.SemaphoreType.DMA((8,))],
    )
    m = CAP * nep
    hidden, downs = call(
        expert_kernel, [((m, f), bf16), ((ntp, f, quarter), bf16)],
        (arrived, expert_gate, expert_up, *downs), in_specs=[VM] * 3 + [HBM] * 4,
        scratch=[pltpu.VMEM((m, d), bf16), pltpu.SemaphoreType.DMA((4,))],
    )
    hiddens = [hidden] + [lax.ppermute(hidden, "tp", around(k, ntp)) for k in range(1, ntp)]
    (column,) = call(stack_kernel, [((8, *joined.shape[1:]), bf16)], (after(near, hidden), *far))
    planes = [column] + [shift(column, 0, k, 0) for k in range(1, 4)]
    blocks = [column, shift(column, 0, 0, 1)]
    (back,) = call(
        down_kernel, [((n_pick, quarter // 2), bf16)], (*hiddens, downs), out_specs=[HBM],
        scratch=[pltpu.VMEM((n_pick, quarter // 2), bf16), pltpu.SemaphoreType.DMA((6,))],
    )
    returned = lax.all_to_all(back.reshape(nep, 8, -1), "ep", 0, 0, tiled=True)
    returned = returned.reshape(n_pick, -1)
    for block in planes[1:]:
        blocks += [block, shift(block, 0, 0, 1)]
    shares = call(
        shared_kernel, [((rows, quarter), f32)] + [((rows, quarter), bf16)] * 3,
        (jnp.stack([lax.axis_index("ep"), part[0]]), after(normed_mix, back), shared_down, residual,
         mix_gate, *blocks),
        in_specs=[SM, VM, VM, HBM] + [VM] * 9,
        scratch=[pltpu.VMEM((rows, d), f32), pltpu.VMEM((rows, quarter), f32), pltpu.SemaphoreType.DMA],
    )
    far_share = lax.ppermute(shares[2], "tp", around(2, ntp))
    shares = [shares[0], far_share] + [lax.ppermute(shares[k], "tp", around(k, ntp)) for k in (1, 3)]
    (layer_out,) = call(
        final_kernel, [((rows, quarter), bf16)],
        (returned, mix, mix_gate, *shares),
    )
    return (layer_out, new_kv)


def solution(mesh):
    placed = (
        P("ep", None), P("ep"), P("ep", None, "tp"), P(), P(None, "tp"), P(None, "tp"), P(None, "tp"),
        P("tp"), P("tp", None), P(), P("ep", None), P("ep", None), P("ep", None, "tp"),
        P("ep", None, "tp"), P("ep", "tp", None), P("ep", "tp"), P("ep", "tp"), P("tp", None), P(),
    )

    return jax.shard_map(shards, mesh=mesh, in_specs=placed, out_specs=(P("ep", "tp"), P("ep", "tp")), check_vma=False)
```
